512 devices in a mesh: ep: 32 (over z, core), tp: 16 (over y, x).
Axes of the slice: x: 4, y: 4, z: 16, core: 2. Of those that a mesh axis runs over, the one named last changes fastest.
Arguments:
- query_rows: bfloat16 [16384, 2048], P('ep', 'tp'), may hold values from -6 to 6
- key_rows: bfloat16 [16384, 2048], P('ep', 'tp'), may hold values from -6 to 6
- value_rows: bfloat16 [16384, 4096], P('ep', 'tp'), may hold values from -6 to 6
- in_gate: float32 [16, 16384], P('tp', 'ep'), may hold values from -120 to 120
- forget_gate: float32 [16, 16384], P('tp', 'ep'), may hold values from -2 to 20
- out_gate: bfloat16 [16384, 4096], P('ep', 'tp'), may hold values from -6 to 6
- head_gain: float32 [4096], P('tp'), may hold values from 0.1 to 1.9
- mix_weight: bfloat16 [4096, 4096], P(None, 'tp'), may hold values from -0.09375 to 0.09375
- expert_input: bfloat16 [8192, 4096], P('ep', 'tp'), may hold values from -30 to 30
- routes: int32 [8192, 2], P('ep'), may hold values from 0 to 31, all different within a row; in each aligned block of 256 rows (0 to 255, 256 to 511, ...) at most 32 rows name the same one
- route_weight: float32 [8192, 2], P('ep'), may hold values from 0.25 to 1.25
- gate_weight: bfloat16 [32, 1024, 4096], P('ep', 'tp'), may hold values from -0.09375 to 0.09375
- up_weight: bfloat16 [32, 1024, 4096], P('ep', 'tp'), may hold values from -0.09375 to 0.09375
- down_weight: bfloat16 [32, 1024, 4096], P('ep', None, 'tp'), may hold values from -0.1875 to 0.1875
Outputs:
- mixer_out: bfloat16 [16384, 4096], P('ep', 'tp')
- expert_out: bfloat16 [8192, 4096], P('ep', 'tp')
The draws below stay inside these ranges and needn't reach their ends.
Inputs may be any that keep to these rules, and one draw needn't show every extreme that they name: `routes`: each row names 2 different experts. In the rows of one device no expert is named by more than 32 rows, and in the rows of some device an expert is named by exactly 32 rows.
All inputs are finite; a program needn't handle non-finite values.
Results may differ from the reference program's by a relative error of at most 0.0057.
Values may be sent and summed in bfloat16 or wider, within the bound.
A program may use at most 128 MiB of HBM per device.

```python
import math
import jax
import jax.numpy as jnp
import numpy as np
from jax import lax

D = 4096
HEADS = 16
QK = 128
FF = 1024
TOP = 2
BLOCK = 64
ROWS_A = 512
ROWS_B = 256
TOKENS_A = 16384
TOKENS_B = 8192
EXPERTS = 32
CAP = 32
N_EP = 32


def draw_in_gate(key, part):
    base = jnp.clip(jax.random.normal(jax.random.fold_in(key, 11), (HEADS, TOKENS_A), jnp.float32), -4.0, 4.0)
    return base


def draw_forget_gate(key, part):
    slow_share = 0.5
    slow_heads = jax.random.bernoulli(jax.random.fold_in(key, 21), slow_share, (HEADS, 1))
    level = jnp.where(slow_heads, math.log(TOKENS_A) + 0.5, 3.5)
    span_total = TOKENS_A // ROWS_A
    drift = jax.random.uniform(jax.random.fold_in(key, 22), (HEADS, span_total), jnp.float32, -1.0, 1.0)
    noise = 0.7 * jnp.clip(jax.random.normal(jax.random.fold_in(key, 23), (HEADS, TOKENS_A), jnp.float32), -4.0, 4.0)
    return level + jnp.repeat(drift, ROWS_A, axis=1) + noise


def draw_expert_input(key, part):
    row_scale = jnp.exp(jax.random.uniform(jax.random.fold_in(key, 31), (TOKENS_B, 1), jnp.float32, -0.7, 0.7))
    base = jnp.clip(jax.random.normal(jax.random.fold_in(key, 34), (TOKENS_B, D), jnp.float32), -4.0, 4.0)
    return (base * row_scale).astype(jnp.bfloat16)


def steps_of(rng, extent, split, low, high):
    loudness, own = 1.0, jax.random.fold_in(rng, 6)
    for axis_at, shards_of in split:
        steps = jnp.exp(jax.random.uniform(jax.random.fold_in(own, axis_at), (shards_of,), jnp.float32, low / len(split), high / len(split)))
        loudness = loudness * jnp.repeat(steps, extent[axis_at] // shards_of).reshape([-1 if axis == axis_at else 1 for axis in range(len(extent))])
    return loudness


def deal_out(key, own, number, rows, count, top, bound, slope):
    order = jax.random.permutation(key, count)
    packed, usual = load_shares(count, rows * top, bound, slope, True), load_shares(count, rows * top, bound, slope, False)
    places = jnp.arange(count)

    def named(tallies, offset_by):
        used = int((tallies > 0).sum())
        fixed = max(1, used // 4)
        shifted = fixed + (places - fixed + offset_by * (used - fixed)) % max(1, count - fixed)
        return jnp.zeros((count,), jnp.int32).at[order[jnp.where(places < fixed, places, shifted)]].set(jnp.asarray(tallies, jnp.int32))

    tallies = jnp.where(number % 4 == 0, named(packed, number // 4), named(usual, number - number // 4 - 1))
    mixed = jax.random.permutation(jax.random.fold_in(own, 3), count)
    donor, taker = mixed[0:count // 2 * 2:2], mixed[1:count // 2 * 2:2]
    room = jnp.minimum(tallies[donor] - 1, bound - tallies[taker]) // 2
    room = jnp.where((donor == order[0]) | (taker == order[0]) | (tallies[taker] == 0), 0, jnp.maximum(room, 0))
    shifted = jax.random.randint(jax.random.fold_in(own, 4), (count // 2,), 0, 1 << 20) % (room + 1)
    tallies = tallies.at[donor].add(-shifted).at[taker].add(shifted)
    labels = jnp.searchsorted(jnp.cumsum(tallies), jnp.arange(rows * top), side="right").astype(jnp.int32)
    listing = labels.reshape(top, rows).T
    listing = listing[jax.random.permutation(jax.random.fold_in(own, 1), rows)]
    offset_by = jax.random.randint(jax.random.fold_in(own, 2), (rows, 1), 0, top)
    return jnp.take_along_axis(listing, (jnp.arange(top)[None, :] + offset_by) % top, axis=1)


def load_shares(amount, total, bound, lean, full):
    weights = [(1 << 20) // math.isqrt(grade ** lean) + 1 for grade in range(1, amount + 1)]
    largest = bound if full else min(bound, max(-(-total // amount), total * weights[0] // sum(weights)))
    least = 1 if total - largest >= amount - 1 else 0
    given, rest = [largest] + [least] * (amount - 1), total - largest - least * (amount - 1)
    while rest > 0:
        free = [i for i in range(1, amount) if given[i] < largest] or [i for i in range(1, amount) if given[i] < bound]
        mass, remaining = sum([weights[i] for i in free]), rest
        for i in free:
            extra = min(bound - given[i], max(1, remaining * weights[i] // mass), rest)
            given[i] = given[i] + extra
            rest = rest - extra
    return np.array(given)


def centred(key, dims, scale, bound, cuts=(), kind=jnp.bfloat16):
    level = steps_of(key, dims, cuts, -0.22, 0.18) if cuts else 1.0
    entries = jax.random.normal(key, dims, jnp.float32) * scale * level
    return jnp.minimum(jnp.maximum(entries, -bound), bound).astype(kind)


def setup_inputs(seed: int = 0) -> dict:
    key_of = jax.random.split(jax.random.key(seed), 15)
    query_rows = centred(key_of[0], (TOKENS_A, HEADS * QK), 1.0, 6.0, ((0, 32), (1, 16)))
    key_rows = centred(key_of[1], (TOKENS_A, HEADS * QK), 1.0, 6.0, ((0, 32), (1, 16)))
    value_rows = centred(key_of[2], (TOKENS_A, D), 1.0, 6.0, ((0, 32), (1, 16)))
    in_gate = draw_in_gate(jax.random.fold_in(key_of[14], 71), 0)
    forget_gate = draw_forget_gate(jax.random.fold_in(key_of[14], 71), 0)
    out_gate = centred(key_of[5], (TOKENS_A, D), 1.0, 6.0, ((0, 32), (1, 16)))
    head_gain = jnp.clip(1.0 + 0.18 * jax.random.normal(key_of[6], (D,), jnp.float32), 0.1, 1.9)
    mix_weight = centred(key_of[7], (D, D), D ** -0.5, 0.09375, ((1, 16),))
    expert_input = draw_expert_input(jax.random.fold_in(key_of[14], 71), 0)
    routes_keys = jax.random.split(jax.random.fold_in(key_of[9], 1), TOKENS_B // ROWS_B)
    routes_turns = jax.random.permutation(jax.random.fold_in(key_of[9], 3), TOKENS_B // ROWS_B)
    routes = jax.vmap(lambda own, number: deal_out(jax.random.fold_in(key_of[9], 2), own, number, ROWS_B, EXPERTS, TOP, CAP, 1))(routes_keys, routes_turns).reshape((TOKENS_B, TOP))
    route_weight = jnp.clip(0.25 + 1.0 * jax.random.uniform(key_of[10], (TOKENS_B, TOP), jnp.float32) ** steps_of(key_of[10], (TOKENS_B, TOP), ((0, 32),), -0.2, 0.2), 0.25, 1.25)
    gate_weight = centred(key_of[11], (EXPERTS, FF, D), D ** -0.5, 0.09375, ((0, 32), (1, 16)))
    up_weight = centred(key_of[12], (EXPERTS, FF, D), D ** -0.5, 0.09375, ((0, 32), (1, 16)))
    down_weight = centred(key_of[13], (EXPERTS, FF, D), FF ** -0.5, 0.1875, ((0, 32), (2, 16)))
    return dict(query_rows=query_rows, key_rows=key_rows, value_rows=value_rows, in_gate=in_gate, forget_gate=forget_gate, out_gate=out_gate, head_gain=head_gain, mix_weight=mix_weight, expert_input=expert_input, routes=routes, route_weight=route_weight, gate_weight=gate_weight, up_weight=up_weight, down_weight=down_weight)


EPSILON = 1e-06
LOG_FLOOR = -1e+30
HIGHEST_PRECISION = lax.Precision.HIGHEST

def combine(first_part, second_part):
    decay_first, max_first, memory_first, normal_first = first_part
    decay_second, max_second, memory_second, normal_second = second_part
    running_max = jnp.maximum(decay_second + max_first, max_second)
    keep_first = jnp.exp(decay_second + max_first - running_max)
    keep_second = jnp.exp(max_second - running_max)
    memory = keep_first[..., None, None] * memory_first + keep_second[..., None, None] * memory_second
    normalizer = keep_first[..., None] * normal_first + keep_second[..., None] * normal_second
    return (decay_first + decay_second, running_max, memory, normalizer)

def identity_state(head_count, key_width, value_width):
    return (jnp.zeros((head_count,), jnp.float32), jnp.full((head_count,), LOG_FLOOR, jnp.float32), jnp.zeros((head_count, key_width, value_width), jnp.float32), jnp.zeros((head_count, key_width), jnp.float32))

def halfprod(form, left, right):
    return jnp.einsum(form, left.astype(jnp.float32), right.astype(jnp.float32), precision=HIGHEST_PRECISION)

def prepare(query_heads, key_heads, value_heads, in_gate, forget_gate):
    head_count, length, key_width = query_heads.shape
    block_count = length // BLOCK
    query_blocks = query_heads.reshape(head_count, block_count, BLOCK, key_width)
    key_blocks = key_heads.reshape(head_count, block_count, BLOCK, key_width)
    value_blocks = value_heads.reshape(head_count, block_count, BLOCK, value_heads.shape[-1])
    log_input = in_gate.reshape(head_count, block_count, BLOCK)
    cumulative = jnp.cumsum(jax.nn.log_sigmoid(forget_gate).reshape(head_count, block_count, BLOCK), axis=-1)
    block_decay = cumulative[..., -1]
    weight_log = block_decay[..., None] - cumulative + log_input
    block_max = lax.optimization_barrier(jnp.max(weight_log, axis=-1))
    weighted = key_blocks.astype(jnp.float32) * jnp.exp(weight_log - block_max[..., None])[..., None]
    normalizer = lax.optimization_barrier(jnp.sum(weighted, axis=2))
    memory = halfprod('hcsk,hcsv->hckv', weighted.astype(jnp.bfloat16), value_blocks)
    return ((query_blocks, key_blocks, value_blocks, log_input, cumulative), (block_decay, block_max, memory, normalizer))

def prefix(summary, initial):
    leading = jax.tree.map(lambda tensor: jnp.moveaxis(tensor, 1, 0), summary)

    def advance(running, current):
        return (combine(running, current), running)
    final_state, before = lax.scan(advance, initial, leading)
    return (final_state, jax.tree.map(lambda tensor: jnp.moveaxis(tensor, 0, 1), before))

def block_outputs(blocked, before):
    query_blocks, key_blocks, value_blocks, log_input, cumulative = blocked
    prior_max, prior_memory, prior_normal = (before[1], before[2], before[3])
    block_len = cumulative.shape[-1]
    scale = query_blocks.shape[-1] ** (-0.5)
    causal = jnp.tril(jnp.ones((block_len, block_len), dtype=bool))
    log_decay = jnp.where(causal, cumulative[..., :, None] - cumulative[..., None, :] + log_input[..., None, :], -jnp.inf)
    log_inter = cumulative + prior_max[..., None]
    top_value = jnp.maximum(log_inter, lax.optimization_barrier(jnp.max(log_decay, axis=-1)))
    scores = halfprod('hctk,hcsk->hcts', query_blocks, key_blocks) * scale * jnp.exp(log_decay - top_value[..., None])
    carried = jnp.exp(log_inter - top_value) * scale
    query_wide = query_blocks.astype(jnp.float32)
    numerator = carried[..., None] * jnp.einsum('hctk,hckv->hctv', query_wide, prior_memory, precision=HIGHEST_PRECISION) + halfprod('hcts,hcsv->hctv', scores.astype(jnp.bfloat16), value_blocks)
    denominator = carried * jnp.einsum('hctk,hck->hct', query_wide, prior_normal, precision=HIGHEST_PRECISION) + lax.optimization_barrier(jnp.sum(scores, axis=-1))
    return numerator / jnp.maximum(jnp.abs(denominator), jnp.exp(-top_value))[..., None]

def finish(head_values, out_gate, head_gain):
    head_count, block_count, block_len, value_width = head_values.shape
    per_head = jnp.transpose(head_values, (1, 2, 0, 3)).reshape(block_count * block_len, head_count, value_width)
    per_head = per_head * lax.rsqrt(lax.optimization_barrier(jnp.mean(per_head * per_head, axis=-1, keepdims=True)) + EPSILON)
    per_head = per_head.reshape(block_count * block_len, head_count * value_width) * head_gain
    per_head = per_head * jax.nn.sigmoid(out_gate.astype(jnp.float32))
    return per_head.astype(jnp.bfloat16)

def reference(query_rows, key_rows, value_rows, in_gate, forget_gate, out_gate, head_gain, mix_weight, expert_input, routes, route_weight, gate_weight, up_weight, down_weight):
    length = query_rows.shape[0]
    head_count = in_gate.shape[0]
    key_width = query_rows.shape[1] // head_count
    value_width = value_rows.shape[1] // head_count
    query_heads = query_rows.reshape(length, head_count, key_width).transpose(1, 0, 2)
    key_heads = key_rows.reshape(length, head_count, key_width).transpose(1, 0, 2)
    value_heads = value_rows.reshape(length, head_count, value_width).transpose(1, 0, 2)

    def one_head(current):
        query_one, key_one, value_one, input_one, forget_one = current
        blocked, summary = prepare(query_one[None], key_one[None], value_one[None], input_one[None], forget_one[None])
        final_state, before = prefix(summary, identity_state(1, key_width, value_width))
        return block_outputs(blocked, before)[0]
    head_values = lax.map(one_head, (query_heads, key_heads, value_heads, in_gate, forget_gate))
    mixed_heads = finish(head_values, out_gate, head_gain)
    mixer_out = jnp.dot(mixed_heads, mix_weight, preferred_element_type=jnp.float32).astype(jnp.bfloat16)
    squares = lax.optimization_barrier(jnp.sum(jnp.square(expert_input.astype(jnp.float32)), axis=-1))
    inverse_rms = lax.rsqrt(squares / D + EPSILON)
    slot_total = N_EP * CAP

    def one_expert(running, expert):
        matched = routes == expert
        picked = jnp.any(matched, axis=1)
        row_index = jnp.nonzero(picked, size=slot_total, fill_value=0)[0].astype(jnp.int32)
        count = jnp.sum(picked.astype(jnp.int32))
        is_valid = (jnp.arange(slot_total, dtype=jnp.int32) < count).astype(jnp.float32)
        weight = lax.optimization_barrier(jnp.sum(jnp.where(matched, route_weight, 0.0), axis=1))
        chosen = expert_input[row_index]
        row_scale = inverse_rms[row_index][:, None]
        gate_value = jnp.dot(chosen, gate_weight[expert].T, preferred_element_type=jnp.float32) * row_scale
        up_value = jnp.dot(chosen, up_weight[expert].T, preferred_element_type=jnp.float32) * row_scale
        hidden = (jax.nn.silu(gate_value) * up_value).astype(jnp.bfloat16)
        expert_rows = jnp.dot(hidden, down_weight[expert], preferred_element_type=jnp.float32).astype(jnp.bfloat16)
        term = expert_rows.astype(jnp.float32) * (weight[row_index] * is_valid)[:, None]
        return (running.at[row_index].add(term), None)
    total, _ = lax.scan(one_expert, jnp.zeros((TOKENS_B, D), jnp.float32), jnp.arange(EXPERTS, dtype=jnp.int32))
    return (mixer_out, total.astype(jnp.bfloat16))
```

```python
import functools

import jax
import jax.numpy as jnp
from jax import lax
from jax.experimental import pallas as pl
from jax.experimental.pallas import tpu as pltpu
from jax.sharding import PartitionSpec as P

EPSILON = 1e-06
LOG_FLOOR = -1e30
F32 = jnp.float32
BF16 = jnp.bfloat16
GROUPS = 4
SIDE = 4
PARTS = 2
CHUNKS = 4
HEAD = 8
HOLD = 4


def flip(index, bits):
    place = 1
    while place <= bits:
        if bits & place:
            index = index + place * (1 - 2 * ((index // place) % 2))
        place *= 2
    return index


def dot(left, right, contract=((1,), (0,))):
    return lax.dot_general(left, right, (contract, ((), ())), preferred_element_type=F32)


def own_mask(size):
    return lax.broadcasted_iota(jnp.int32, (size, size), 0) == lax.broadcasted_iota(
        jnp.int32, (size, size), 1
    )


def upright(row):
    size = row.shape[1]
    return jnp.sum(jnp.where(own_mask(size), row, 0.0), axis=1, keepdims=True)


def flat(column):
    size = column.shape[0]
    return jnp.sum(jnp.where(own_mask(size), column, 0.0), axis=0, keepdims=True)


def kernel(
    ep,
    tp,
    model_width,
    x_ref,
    slot_row_ref,
    weight_ref,
    a_ref,
    cum_ref,
    gain_ref,
    q_hbm,
    k_hbm,
    v_hbm,
    og_hbm,
    wg_hbm,
    wu_hbm,
    wd_hbm,
    wm_hbm,
    mix_ref,
    exp_ref,
    q_ref,
    k_ref,
    v_ref,
    og_ref,
    wd_ref,
    wm_ref,
    wm_turned,
    w1,
    w2,
    slots,
    tok,
    part_own,
    part_out,
    part_in,
    sq_out,
    sq_in,
    hid,
    outb,
    ret,
    hm,
    num_ref,
    den_ref,
    top_ref,
    loc,
    pair_in,
    both,
    st_in,
    st_out,
    prior,
    load_sem,
    own_sem,
    deal_send,
    deal_recv,
    disp_send,
    disp_recv,
    tok_send,
    tok_recv,
    part_send,
    part_recv,
    sq_send,
    sq_recv,
    hid_send,
    hid_recv,
    ret_send,
    ret_recv,
    head_send,
    head_recv,
    pair_send,
    pair_recv,
    down_send,
    down_recv,
    st_send,
    st_recv,
):
    me = lax.axis_index("ep")
    mine = lax.axis_index("tp")
    row, column = mine // SIDE, mine % SIDE
    chip, core = me // 2, me % 2
    chips = ep // 2
    cap = slots.shape[0] // ep
    span = slots.shape[0] // GROUPS
    half_span = span // 2
    per = ep // GROUPS
    width = x_ref.shape[1]
    tokens = x_ref.shape[0]
    length, qk = q_ref.shape
    vw = v_ref.shape[1]
    units = wg_hbm.shape[0]
    wide = SIDE * width
    last = chips - 1

    loads = [
        pltpu.make_async_copy(source, target, load_sem.at[at])
        for at, (source, target) in enumerate(
            [
                (k_hbm, k_ref),
                (v_hbm, v_ref),
                (q_hbm, q_ref),
                (og_hbm, og_ref),
                (wd_hbm, wd_ref),
                (wm_hbm, wm_ref),
            ]
        )
    ]
    for load in loads:
        load.start()

    def piece(source, j, k):
        start = pl.multiple_of((flip(row, k) * SIDE + flip(column, j)) * width, width)
        return source.at[:, pl.ds(start, width)]

    def slot_of(j, which, k):
        return w1.at[pl.ds((2 * j + which) * units, units), pl.ds(k * width, width)]

    own_pieces = [
        pltpu.make_async_copy(
            piece(source, 0, k), slot_of(0, which, k), own_sem.at[which * SIDE + k]
        )
        for which, source in enumerate((wg_hbm, wu_hbm))
        for k in range(SIDE)
    ]
    for load in own_pieces:
        load.start()

    def deal(j, which, k):
        at = (j - 1) * 2 * SIDE + which * SIDE + k
        return pltpu.make_async_remote_copy(
            piece(wu_hbm if which else wg_hbm, j, k),
            slot_of(j, which, k),
            deal_send.at[at],
            deal_recv.at[at],
            device_id={"tp": flip(mine, j)},
        )

    dealt = [(j, which, k) for j in range(1, SIDE) for which in range(2) for k in range(SIDE)]

    barrier = pltpu.get_barrier_semaphore()
    for i in range(1, ep):
        pl.semaphore_signal(barrier, inc=1, device_id={"ep": flip(me, i)})
    for j in range(1, tp):
        pl.semaphore_signal(barrier, inc=1, device_id={"tp": flip(mine, j)})

    def pick(group, carry):
        at = group * span
        rows = at + lax.broadcasted_iota(jnp.int32, (span, tokens), 0)
        hit = (rows == slot_row_ref[0:1, :]) | (rows == slot_row_ref[1:2, :])
        chosen = dot(hit.astype(F32).astype(BF16), x_ref[...]).astype(BF16)
        slots[pl.ds(pl.multiple_of(at, span), span), :] = chosen
        return carry

    lax.fori_loop(0, GROUPS, pick, 0)

    loads[0].wait()
    loads[1].wait()
    decay = cum_ref[0:1, length - 1 : length]
    log_in = a_ref[0:1, :]
    local_top = jnp.max(log_in, axis=1, keepdims=True)
    weighted = k_ref[...].astype(F32) * jnp.exp(upright(log_in) - local_top)
    loc[HEAD : HEAD + qk, :] = dot(weighted.astype(BF16), v_ref[...], ((0,), (0,)))
    loc[0:HEAD, 0:qk] = jnp.broadcast_to(jnp.sum(weighted, axis=0, keepdims=True), (HEAD, qk))
    loc[0:HEAD, qk:vw] = jnp.broadcast_to(local_top + decay, (HEAD, vw - qk))
    loc[HEAD + qk :, :] = jnp.broadcast_to(decay, (8, vw))

    @pl.when(chip == 0)
    def _():
        st_in[0:HEAD, 0:qk] = jnp.zeros((HEAD, qk), F32)
        st_in[0:HEAD, qk:vw] = jnp.full((HEAD, vw - qk), LOG_FLOOR, F32)
        st_in[HEAD:, :] = jnp.zeros((qk, vw), F32)

    pl.semaphore_wait(barrier, ep - 1 + tp - 1)

    pair = pltpu.make_async_remote_copy(
        loc, pair_in, pair_send.at[0], pair_recv.at[0], device_id={"ep": flip(me, 1)}
    )

    @pl.when(core == 0)
    def _():
        pair.start()

    def dispatch(i):
        return pltpu.make_async_remote_copy(
            slots.at[pl.ds(i * cap, cap)],
            tok.at[pl.ds(i * cap, cap), pl.ds(0, width)],
            disp_send.at[i],
            disp_recv.at[i],
            device_id={"ep": flip(me, i)},
        )

    def held(i):
        ahead = (flip(chip, i // 2) - chip + chips) % chips
        return (core == 1) & (chip < HOLD) & (ahead > 0) & (ahead <= chips // 2)

    for i in range(1, ep):

        @pl.when(jnp.logical_not(held(i)))
        def _():
            dispatch(i).start()

    tok[0:cap, 0:width] = slots[0:cap, :]
    for each in dealt:
        deal(*each).start()

    def gates(first_max, second_max):
        top = jnp.maximum(first_max, second_max)
        return top, jnp.exp(first_max - top), jnp.exp(second_max - top)

    def merge(target, lower, upper, keep, add, top):
        if lower == 0:
            first, second = target[1], target[2]
            target[0][0:HEAD, 0:qk] = keep * first[0:HEAD, 0:qk] + add * second[0:HEAD, 0:qk]
            target[0][0:HEAD, qk:vw] = jnp.broadcast_to(top, (HEAD, vw - qk))
            lower = HEAD
        target[0][lower:upper, :] = (
            keep * target[1][lower:upper, :] + add * target[2][lower:upper, :]
        )

    edges = [0] + [HEAD + (at + 1) * (qk // CHUNKS) for at in range(CHUNKS)]

    def chain(at):
        rows = pl.ds(edges[at], edges[at + 1] - edges[at])
        return pltpu.make_async_remote_copy(
            st_out.at[rows],
            st_in.at[rows],
            st_send.at[at],
            st_recv.at[at],
            device_id={"ep": me + 2},
        )

    def down(at):
        rows = pl.ds(edges[at], edges[at + 1] - edges[at])
        return pltpu.make_async_remote_copy(
            st_in.at[rows],
            st_in.at[rows],
            down_send.at[at],
            down_recv.at[at],
            device_id={"ep": flip(me, 1)},
        )

    @pl.when(core == 1)
    def _():
        pair.wait_recv()
        top, keep, add = gates(
            pair_in[0:1, qk : qk + 1] + decay,
            loc[0:1, qk : qk + 1],
        )
        merge((both, pair_in, loc), 0, HEAD + qk, keep, add, top)

    def chain_step():
        both_decay = pair_in[HEAD + qk : HEAD + qk + 1, 0:1] + decay
        keep = add = top = None
        for at in range(CHUNKS):

            @pl.when(chip > 0)
            def _():
                chain(at).wait_recv()
                down(at).start()

            if at == 0:
                top, keep, add = gates(
                    st_in[0:1, qk : qk + 1] + both_decay, both[0:1, qk : qk + 1]
                )

            merge((st_out, st_in, both), edges[at], edges[at + 1], keep, add, top)

            @pl.when(chip < last)
            def _():
                chain(at).start()

    ticks = GROUPS + 7

    def chain_slot(tick):
        turn = jnp.maximum(chip * 5 // 8 - 1, -1)

        @pl.when((core == 1) & (turn == tick))
        def _():
            chain_step()

    chain_slot(-1)

    loads[2].wait()
    tile = length // 4
    scale = qk**-0.5
    for at in range(4):
        rows = pl.ds(at * tile, tile)
        seen = (at + 1) * tile
        causal = lax.broadcasted_iota(jnp.int32, (tile, seen), 1) <= at * tile + (
            lax.broadcasted_iota(jnp.int32, (tile, seen), 0)
        )
        log_seen = jnp.where(causal, a_ref[0:1, 0:seen], -jnp.inf)
        top = jnp.max(log_seen, axis=1, keepdims=True)
        scores = dot(q_ref[rows, :], k_ref[0:seen, :], ((1,), (1,))) * scale
        scores = scores * jnp.exp(log_seen - top)
        num_ref[rows, :] = dot(scores.astype(BF16), v_ref[0:seen, :])
        den_ref[rows, :] = jnp.broadcast_to(jnp.sum(scores, axis=1, keepdims=True), (tile, 128))
        top_ref[rows, :] = jnp.broadcast_to(top, (tile, 128))

    loads[4].wait()
    nothing = jnp.zeros((units, width), BF16)
    for turned in range(2):
        for at in range(tp):
            unit = (at % SIDE) * SIDE + at // SIDE if turned else at
            block = wd_ref[unit * units : (unit + 1) * units, :]
            first = at * 2 * units
            w2[turned, first : first + units, 0:width] = block
            w2[turned, first : first + units, width : 2 * width] = nothing
            w2[turned, first + units : first + 2 * units, 0:width] = nothing
            w2[turned, first + units : first + 2 * units, width : 2 * width] = block
    loads[5].wait()

    def turn_block(at, carry):
        source = pl.multiple_of(((at % SIDE) * SIDE + at // SIDE) * width, width)
        target = pl.multiple_of(at * width, width)
        wm_turned[pl.ds(target, width), :] = wm_ref[pl.ds(source, width), :]
        return carry

    lax.fori_loop(0, tp, turn_block, 0)


    def spread(group, k):
        rows = pl.ds(group * span, span)
        return pltpu.make_async_remote_copy(
            tok.at[rows, pl.ds(0, width)],
            tok.at[rows, pl.ds(k * width, width)],
            tok_send.at[group, k],
            tok_recv.at[group, k],
            device_id={"tp": flip(mine, SIDE * k)},
        )

    def onward(group, k):
        rows = pl.ds(group * span + (k // 2) * half_span, half_span)
        return pltpu.make_async_remote_copy(
            tok.at[rows, pl.ds(k * width, width)],
            tok.at[rows, pl.ds(2 * width, width)],
            tok_send.at[group, 4 + k],
            tok_recv.at[group, 4 + k],
            device_id={"tp": flip(mine, SIDE * (SIDE - k))},
        )

    def send_partial(group, j):
        rows = pl.ds(group * span, span)
        return pltpu.make_async_remote_copy(
            part_out.at[j, rows],
            part_in.at[j, rows],
            part_send.at[group, j],
            part_recv.at[group, j],
            device_id={"tp": flip(mine, j)},
        )

    def send_squares(group, j):
        return pltpu.make_async_remote_copy(
            sq_out.at[group],
            sq_in.at[group, j],
            sq_send.at[group, j],
            sq_recv.at[group, j],
            device_id={"tp": flip(mine, j)},
        )


    def gather_copies(buffer, first_row, rows, wide_block, x_first, send, recv):
        inner, outer = (column, row) if x_first else (row, column)
        inner_bits, outer_bits = (1, SIDE) if x_first else (SIDE, 1)
        base = outer * SIDE * wide_block
        half = rows // 2

        def cut(part, block, count):
            begin, extent = (first_row, rows) if part is None else (first_row + part * half, half)
            return buffer.at[
                pl.ds(begin, extent),
                pl.ds(pl.multiple_of(base + block * wide_block, wide_block), count * wide_block),
            ]

        def outer_cut(part, bits):
            begin, extent = (first_row, rows) if part is None else (first_row + part * half, half)
            start = pl.multiple_of(flip(outer, bits) * SIDE * wide_block, SIDE * wide_block)
            return buffer.at[pl.ds(begin, extent), pl.ds(start, SIDE * wide_block)]

        def remote(piece_of, at, bits):
            return pltpu.make_async_remote_copy(
                piece_of, piece_of, send.at[at], recv.at[at], device_id={"tp": flip(mine, bits)}
            )

        def inner_send(k):
            return remote(cut(None, inner, 1), k // 2, k * inner_bits)

        def inner_relay(k):
            return remote(
                cut(k // 2, flip(inner, k), 1), 2 + k // 2, (SIDE - k) * inner_bits
            )

        def outer_send(k):
            return remote(outer_cut(None, 0), 4 + k // 2, k * outer_bits)

        def outer_relay(k):
            return remote(outer_cut(k // 2, k), 6 + k // 2, (SIDE - k) * outer_bits)

        return [[make(k) for k in (1, 3)] for make in (inner_send, inner_relay, outer_send, outer_relay)]

    def gather_step(copies, step):
        if step > 0:
            for copy in copies[step - 1]:
                copy.wait_recv()
        if step < 4:
            for copy in copies[step]:
                copy.start()

    hid_copies = [
        gather_copies(
            hid,
            group * half_span,
            half_span,
            2 * units,
            group % 2 == 0,
            hid_send.at[group],
            hid_recv.at[group],
        )
        for group in range(GROUPS)
    ]

    def give_back(i):
        return pltpu.make_async_remote_copy(
            outb.at[pl.ds(i * cap, cap)],
            ret.at[pl.ds(i * cap, cap)],
            ret_send.at[i],
            ret_recv.at[i],
            device_id={"ep": flip(me, i)},
        )

    def stage(group, step):
        rows = pl.ds(group * span, span)
        packed = pl.ds(group * half_span, half_span)
        if step == 0:
            for i in range(max(1, group * per), (group + 1) * per):
                dispatch(i).wait_recv()
            for k in (1, 3):
                spread(group, k).start()
        elif step == 1:
            for k in (1, 3):
                spread(group, k).wait_recv()
                onward(group, k).start()
        elif step == 2:
            if group == 0:
                for load in own_pieces:
                    load.wait()
                for each in dealt:
                    deal(*each).wait_recv()
            for k in (1, 3):
                onward(group, k).wait_recv()
            piece_of = tok[rows, :]
            partial = dot(piece_of, w1[...], ((1,), (1,)))
            part_own[rows, :] = partial[:, 0 : 2 * units]
            for j in range(1, SIDE):
                part_out[j, rows, :] = partial[:, j * 2 * units : (j + 1) * 2 * units].astype(BF16)
            for j in range(1, SIDE):
                send_partial(group, j).start()
            full = piece_of.astype(F32)
            squares = flat(jnp.sum(full * full, axis=1, keepdims=True))
            sq_out[group] = jnp.broadcast_to(squares, (8, span))
            for j in range(1, SIDE):
                send_squares(group, j).start()
        elif step == 3:
            squares = sq_out[group][0:1, :]
            for j in range(1, SIDE):
                send_squares(group, j).wait_recv()
                squares = squares + sq_in[group, j][0:1, :]
            inverse = upright(lax.rsqrt(squares / model_width + EPSILON))
            total = part_own[rows, :]
            for j in range(1, SIDE):
                send_partial(group, j).wait_recv()
                total = total + part_in[j, rows, :].astype(F32)
            total = total * inverse
            hidden = jax.nn.silu(total) * pltpu.roll(total, units, 1)
            turned = pltpu.roll(hidden, units, 1)
            lanes = lax.broadcasted_iota(jnp.int32, (half_span, 2 * units), 1)
            both_rows = jnp.where(lanes < units, hidden[0:half_span, :], turned[half_span:span, :])
            place = mine if group % 2 == 0 else column * SIDE + row
            columns = pl.ds(pl.multiple_of(place * 2 * units, 2 * units), 2 * units)
            hid[packed, columns] = both_rows.astype(BF16)
            gather_step(hid_copies[group], 0)
        elif step < 7:
            gather_step(hid_copies[group], step - 3)
        else:
            gather_step(hid_copies[group], 4)
            total = dot(hid[packed, :], w2[group % 2])
            outb[pl.ds(group * span, half_span), :] = total[:, 0:width].astype(BF16)
            outb[pl.ds(group * span + half_span, half_span), :] = total[:, width:].astype(BF16)
            for i in range(max(1, group * per), (group + 1) * per):
                give_back(i).start()

    for tick in range(ticks):
        if tick < 9:
            chain_slot(tick)
        if tick == 0:
            for i in range(1, ep):

                @pl.when(held(i))
                def _():
                    dispatch(i).start()

        for group in range(GROUPS):
            if 0 <= tick - group < 8:
                stage(group, tick - group)
    ret[0:cap, :] = outb[0:cap, :]


    @pl.when((core == 0) & (chip > 0))
    def _():
        for at in range(CHUNKS):
            down(at).wait_recv()

    @pl.when(core == 0)
    def _():
        prior[...] = st_in[...]

    @pl.when(core == 1)
    def _():
        other_decay = pair_in[HEAD + qk : HEAD + qk + 1, 0:1]
        top, keep, add = gates(
            st_in[0:1, qk : qk + 1] + other_decay, pair_in[0:1, qk : qk + 1]
        )
        merge((prior, st_in, pair_in), 0, HEAD + qk, keep, add, top)

    loads[3].wait()
    part_rows = length // (2 * PARTS)
    head_copies = [
        gather_copies(
            hm.at[at // PARTS],
            (at % PARTS) * part_rows,
            part_rows,
            width,
            at // PARTS == 0,
            head_send.at[at],
            head_recv.at[at],
        )
        for at in range(2 * PARTS)
    ]
    prior_max = prior[0:1, qk : qk + 1]
    normal = prior[0:1, 0:qk]
    memory = prior[HEAD:, :]
    high = memory.astype(BF16)
    low = (memory - high.astype(F32)).astype(BF16)
    for order in range(2 * PARTS):
        at = order // 2 + (order % 2) * PARTS
        rows = pl.ds(at * part_rows, part_rows)
        queries = q_ref[rows, :]
        own_top = top_ref[rows, 0:1]
        top = jnp.maximum(prior_max, own_top)
        again = jnp.exp(own_top - top)
        carried = jnp.exp(prior_max - top) * scale
        numerator = carried * (dot(queries, high) + dot(queries, low)) + again * num_ref[rows, :]
        denominator = (
            carried * jnp.sum(queries.astype(F32) * normal, axis=1, keepdims=True)
            + again * den_ref[rows, 0:1]
        )
        cumulative = upright(cum_ref[0:1, at * part_rows : (at + 1) * part_rows])
        floor = jnp.exp(-(cumulative + top))
        value = numerator / jnp.maximum(jnp.abs(denominator), floor)
        value = value * lax.rsqrt(jnp.mean(value * value, axis=1, keepdims=True) + EPSILON)
        gate = jax.nn.sigmoid(og_ref[rows, :].astype(F32))
        place = mine if at < PARTS else column * SIDE + row
        hm[
            at // PARTS,
            pl.ds((at % PARTS) * part_rows, part_rows),
            pl.ds(pl.multiple_of(place * width, width), width),
        ] = (value * gain_ref[...] * gate).astype(BF16)
        gather_step(head_copies[at], 0)

    for step in range(1, 5):
        for order in range(2 * PARTS):
            at = order // 2 + (order % 2) * PARTS
            gather_step(head_copies[at], step)
            if step == 4:
                inputs = hm[at // PARTS, pl.ds((at % PARTS) * part_rows, part_rows), :]
                weights = wm_ref if at < PARTS else wm_turned
                mix_ref[pl.ds(at * part_rows, part_rows), :] = dot(inputs, weights[...]).astype(BF16)

    total = jnp.zeros((tokens, width), F32)
    places = lax.broadcasted_iota(jnp.int32, (span, tokens), 0)
    weights = [upright(weight_ref[route : route + 1, :]) for route in range(weight_ref.shape[0])]
    for group in range(GROUPS):
        for i in range(max(1, group * per), (group + 1) * per):
            give_back(i).wait_recv()
        rows = pl.ds(group * span, span)
        for route, weight in enumerate(weights):
            hit = places == slot_row_ref[route : route + 1, :] - group * span
            picked = dot(hit.astype(F32).astype(BF16), ret[rows, :], ((0,), (0,)))
            total += picked * weight
    exp_ref[...] = total.astype(BF16)

    for i in range(1, ep):
        dispatch(i).wait_send()
        give_back(i).wait_send()
    for each in dealt:
        deal(*each).wait_send()
    for group in range(GROUPS):
        for k in (1, 3):
            spread(group, k).wait_send()
            onward(group, k).wait_send()
        for j in range(1, SIDE):
            send_partial(group, j).wait_send()
            send_squares(group, j).wait_send()
    for copies in hid_copies + head_copies:
        for step in copies:
            for copy in step:
                copy.wait_send()

    @pl.when(core == 0)
    def _():
        pair.wait_send()

    for at in range(CHUNKS):

        @pl.when((core == 1) & (chip > 0))
        def _():
            down(at).wait_send()

        @pl.when((core == 1) & (chip < last))
        def _():
            chain(at).wait_send()


def body(
    query_rows,
    key_rows,
    value_rows,
    in_gate,
    forget_gate,
    out_gate,
    head_gain,
    mix_weight,
    expert_input,
    routes,
    route_weight,
    gate_weight,
    up_weight,
    down_weight,
):
    ep, tp = lax.axis_size("ep"), lax.axis_size("tp")
    length = in_gate.shape[1]
    token_count, fanout = routes.shape
    width = expert_input.shape[1]
    units = gate_weight.shape[1]
    capacity = 2 * token_count * fanout // ep
    slot_count = ep * capacity
    qk = query_rows.shape[1]
    vw = value_rows.shape[1]

    earlier = jnp.tril(jnp.ones((length, length), F32))
    cumulative = jnp.einsum(
        "hs,ts->ht", jax.nn.log_sigmoid(forget_gate), earlier, precision=lax.Precision.HIGHEST
    )
    shifted = in_gate - cumulative

    me = lax.axis_index("ep")
    turned = routes ^ me
    experts = jnp.arange(ep, dtype=jnp.int32)
    named = turned[:, :, None] == experts
    any_named = jnp.any(named, axis=1)
    before = jnp.dot(
        jnp.tril(jnp.ones((token_count, token_count), BF16), -1),
        any_named.astype(BF16),
        preferred_element_type=F32,
    ).astype(jnp.int32)
    places = experts * capacity + before
    slot_row = jnp.sum(jnp.where(named, places[:, None, :], 0), axis=2).T

    vmem = pl.BlockSpec(memory_space=pltpu.VMEM)
    anywhere = pl.BlockSpec(memory_space=pl.ANY)
    dma = pltpu.SemaphoreType.DMA
    gate_local, up_local, down_local = gate_weight[0], up_weight[0], down_weight[0]
    big = (query_rows, key_rows, value_rows, out_gate, gate_local, up_local, down_local, mix_weight)
    held = (query_rows, key_rows, value_rows, out_gate, down_local, mix_weight, mix_weight)
    deals = (SIDE - 1) * 2 * SIDE
    state = (HEAD + qk, vw)
    tall = (HEAD + qk + 8, vw)
    return pl.pallas_call(
        functools.partial(kernel, ep, tp, mix_weight.shape[0]),
        out_shape=(
            jax.ShapeDtypeStruct((length, width), BF16),
            jax.ShapeDtypeStruct((token_count, width), BF16),
        ),
        in_specs=[vmem] * 6 + [anywhere] * 8,
        out_specs=(vmem, vmem),
        scratch_shapes=[pltpu.VMEM(array.shape, array.dtype) for array in held]
        + [
            pltpu.VMEM((SIDE * 2 * units, SIDE * width), BF16),
            pltpu.VMEM((2, tp * 2 * units, 2 * width), BF16),
            pltpu.VMEM((slot_count, width), BF16),
            pltpu.VMEM((slot_count, SIDE * width), BF16),
            pltpu.VMEM((slot_count, 2 * units), F32),
            pltpu.VMEM((SIDE, slot_count, 2 * units), BF16),
            pltpu.VMEM((SIDE, slot_count, 2 * units), BF16),
            pltpu.VMEM((GROUPS, 8, slot_count // GROUPS), F32),
            pltpu.VMEM((GROUPS, SIDE, 8, slot_count // GROUPS), F32),
            pltpu.VMEM((slot_count // 2, tp * 2 * units), BF16),
            pltpu.VMEM((slot_count, width), BF16),
            pltpu.VMEM((slot_count, width), BF16),
            pltpu.VMEM((2, length // 2, tp * width), BF16),
            pltpu.VMEM((length, vw), F32),
            pltpu.VMEM((length, 128), F32),
            pltpu.VMEM((length, 128), F32),
            pltpu.VMEM(tall, F32),
            pltpu.VMEM(tall, F32),
            pltpu.VMEM(state, F32),
            pltpu.VMEM(state, F32),
            pltpu.VMEM(state, F32),
            pltpu.VMEM(state, F32),
            dma((6,)),
            dma((2 * SIDE,)),
            dma((deals,)),
            dma((deals,)),
            dma((ep,)),
            dma((ep,)),
            dma((GROUPS, 8)),
            dma((GROUPS, 8)),
            dma((GROUPS, SIDE)),
            dma((GROUPS, SIDE)),
            dma((GROUPS, SIDE)),
            dma((GROUPS, SIDE)),
            dma((GROUPS, 8)),
            dma((GROUPS, 8)),
            dma((ep,)),
            dma((ep,)),
            dma((2 * PARTS, 8)),
            dma((2 * PARTS, 8)),
            dma((1,)),
            dma((1,)),
            dma((CHUNKS,)),
            dma((CHUNKS,)),
            dma((CHUNKS,)),
            dma((CHUNKS,)),
        ],
        compiler_params=pltpu.CompilerParams(
            collective_id=0, has_side_effects=True, vmem_limit_bytes=64000 * 1024
        ),
    )(
        expert_input,
        slot_row,
        route_weight.T,
        shifted,
        cumulative,
        head_gain[None, :],
        *big,
    )


def solution(mesh):
    in_specs = (
        P("ep", "tp"),
        P("ep", "tp"),
        P("ep", "tp"),
        P("tp", "ep"),
        P("tp", "ep"),
        P("ep", "tp"),
        P("tp"),
        P(None, "tp"),
        P("ep", "tp"),
        P("ep", None),
        P("ep", None),
        P("ep", "tp", None),
        P("ep", "tp", None),
        P("ep", None, "tp"),
    )
    out_specs = (P("ep", "tp"), P("ep", "tp"))
    return jax.shard_map(body, mesh=mesh, in_specs=in_specs, out_specs=out_specs, check_vma=False)
```

```python
import functools

import jax
import jax.numpy as jnp
from jax import lax
from jax.experimental import pallas as pl
from jax.experimental.pallas import tpu as pltpu
from jax.sharding import PartitionSpec as P

EPSILON = 1e-06
LOG_FLOOR = -1e30
F32 = jnp.float32
BF16 = jnp.bfloat16
GROUPS = 4
SIDE = 4
PARTS = 2
BLOCK = 4
HEAD = 8
LABEL = 16
FINISH = 5


def flip(index, bits):
    place = 1
    while place <= bits:
        if bits & place:
            index = index + place * (1 - 2 * ((index // place) % 2))
        place *= 2
    return index


def dot(left, right, contract=((1,), (0,))):
    return lax.dot_general(left, right, (contract, ((), ())), preferred_element_type=F32)


def own_mask(size):
    return lax.broadcasted_iota(jnp.int32, (size, size), 0) == lax.broadcasted_iota(
        jnp.int32, (size, size), 1
    )


def upright(row):
    size = row.shape[1]
    return jnp.sum(jnp.where(own_mask(size), row, 0.0), axis=1, keepdims=True)


def flat(column):
    size = column.shape[0]
    return jnp.sum(jnp.where(own_mask(size), column, 0.0), axis=0, keepdims=True)


def kernel(
    ep,
    tp,
    model_width,
    x_hbm,
    routes_hbm,
    weight_hbm,
    in_hbm,
    forget_hbm,
    gain_hbm,
    q_hbm,
    k_hbm,
    v_hbm,
    og_hbm,
    wg_hbm,
    wu_hbm,
    wd_hbm,
    wm_hbm,
    mix_ref,
    exp_ref,
    x_ref,
    routes_ref,
    weight_ref,
    in_ref,
    forget_ref,
    gain_ref,
    q_ref,
    k_ref,
    v_ref,
    og_ref,
    wd_ref,
    wm_ref,
    slot_row_ref,
    a_ref,
    cum_ref,
    wm_turned,
    w1,
    w2,
    slots,
    tok,
    part_own,
    part_out,
    part_in,
    sq_out,
    sq_in,
    hid,
    outb,
    ret,
    hm,
    num_ref,
    den_ref,
    top_ref,
    loc,
    pair_in,
    both,
    earlier,
    other,
    prior,
    down_in,
    near_out,
    near_in,
    carry_out,
    carry_in,
    load_sem,
    own_sem,
    deal_send,
    deal_recv,
    disp_send,
    disp_recv,
    tok_send,
    tok_recv,
    part_send,
    part_recv,
    sq_send,
    sq_recv,
    hid_send,
    hid_recv,
    ret_send,
    ret_recv,
    head_send,
    head_recv,
    pair_send,
    pair_recv,
    down_send,
    down_recv,
    near_send,
    near_recv,
    carry_send,
    carry_recv,
):
    me = lax.axis_index("ep")
    mine = lax.axis_index("tp")
    row, column = mine // SIDE, mine % SIDE
    chip, core = me // 2, me % 2
    chips = ep // 2
    block, place_in_block = chip // BLOCK, chip % BLOCK
    last_block = chips // BLOCK - 1
    cap = slots.shape[0] // ep
    span = slots.shape[0] // GROUPS
    half_span = span // 2
    per = ep // GROUPS
    width = x_ref.shape[1]
    tokens = x_ref.shape[0]
    length, qk = q_ref.shape
    vw = v_ref.shape[1]
    units = wg_hbm.shape[0]
    wide = SIDE * width

    names = (
        (routes_hbm, routes_ref),
        (x_hbm, x_ref),
        (forget_hbm, forget_ref),
        (in_hbm, in_ref),
        (k_hbm, k_ref),
        (v_hbm, v_ref),
        (q_hbm, q_ref),
        (wd_hbm, wd_ref),
        (wm_hbm, wm_ref),
        (og_hbm, og_ref),
        (gain_hbm, gain_ref),
        (weight_hbm, weight_ref),
    )
    loads = [
        pltpu.make_async_copy(source, target, load_sem.at[at])
        for at, (source, target) in enumerate(names)
    ]
    for load in loads:
        load.start()

    def piece(source, j, k):
        start = pl.multiple_of((flip(row, k) * SIDE + flip(column, j)) * width, width)
        return source.at[:, pl.ds(start, width)]

    def slot_of(j, which, k):
        return w1.at[pl.ds((2 * j + which) * units, units), pl.ds(k * width, width)]

    own_pieces = [
        pltpu.make_async_copy(
            piece(source, 0, k), slot_of(0, which, k), own_sem.at[which * SIDE + k]
        )
        for which, source in enumerate((wg_hbm, wu_hbm))
        for k in range(SIDE)
    ]
    for load in own_pieces:
        load.start()

    def deal(j, which, k):
        return pltpu.make_async_remote_copy(
            piece(wu_hbm if which else wg_hbm, j, k),
            slot_of(j, which, k),
            deal_send.at[0],
            deal_recv.at[0],
            device_id={"tp": flip(mine, j)},
        )

    def deals():
        foreign = w1.at[pl.ds(2 * units, 2 * (SIDE - 1) * units)]
        return pltpu.make_async_remote_copy(
            foreign, foreign, deal_send.at[0], deal_recv.at[0], device_id={"tp": flip(mine, 1)}
        )

    dealt = [(j, which, k) for j in range(1, SIDE) for which in range(2) for k in range(SIDE)]

    barrier = pltpu.get_barrier_semaphore()
    for i in range(1, ep):
        pl.semaphore_signal(barrier, inc=1, device_id={"ep": flip(me, i)})
    for j in range(1, tp):
        pl.semaphore_signal(barrier, inc=1, device_id={"tp": flip(mine, j)})

    loads[0].wait()
    experts = lax.broadcasted_iota(jnp.int32, (ep, tokens), 0)
    named = [experts == (routes_ref[route : route + 1, :] ^ me) for route in range(2)]
    any_named = (named[0] | named[1]).astype(F32).astype(BF16)
    older = lax.broadcasted_iota(jnp.int32, (tokens, tokens), 0) < lax.broadcasted_iota(
        jnp.int32, (tokens, tokens), 1
    )
    before = dot(any_named, older.astype(F32).astype(BF16))
    places = (experts * cap).astype(F32) + before
    for route in range(2):
        slot_row_ref[route : route + 1, :] = jnp.sum(
            jnp.where(named[route], places, 0.0), axis=0, keepdims=True
        ).astype(jnp.int32)
    loads[1].wait()

    def pick(group, carry):
        at = group * span
        rows = at + lax.broadcasted_iota(jnp.int32, (span, tokens), 0)
        hit = (rows == slot_row_ref[0:1, :]) | (rows == slot_row_ref[1:2, :])
        chosen = dot(hit.astype(F32).astype(BF16), x_ref[...]).astype(BF16)
        slots[pl.ds(pl.multiple_of(at, span), span), :] = chosen
        return carry

    lax.fori_loop(0, GROUPS, pick, 0)

    with jax.named_scope("barrier"):
        pl.semaphore_wait(barrier, ep - 1 + tp - 1)

    def dispatch(i):
        return pltpu.make_async_remote_copy(
            slots.at[pl.ds(i * cap, cap)],
            tok.at[pl.ds(i * cap, cap), pl.ds(0, width)],
            disp_send.at[0],
            disp_recv.at[i // per],
            device_id={"ep": flip(me, i)},
        )

    def dispatched(group):
        begin = cap if group == 0 else group * span
        rows = pl.ds(begin, (group + 1) * span - begin)
        return pltpu.make_async_remote_copy(
            slots.at[rows],
            tok.at[rows, pl.ds(0, width)],
            disp_send.at[0],
            disp_recv.at[group],
            device_id={"ep": flip(me, 1)},
        )

    def held(i):
        ahead = (flip(chip, i // 2) - chip + chips) % chips
        return (core == 1) & (place_in_block < BLOCK - 1) & (ahead > 0) & (ahead <= chips // 2)

    for i in range(1, ep):

        @pl.when(jnp.logical_not(held(i)))
        def _():
            dispatch(i).start()

    tok[0:cap, 0:width] = slots[0:cap, :]
    for each in dealt:
        deal(*each).start()


    loads[2].wait()
    loads[3].wait()
    gates_in = forget_ref[...]
    log_keep = jnp.minimum(gates_in, 0.0) - jnp.log1p(jnp.exp(-jnp.abs(gates_in)))
    high = log_keep.astype(BF16).astype(F32)
    mid = (log_keep - high).astype(BF16).astype(F32)
    low = log_keep - high - mid
    which_row = lax.broadcasted_iota(jnp.int32, (8, length), 0)
    thirds = jnp.where(
        which_row == 0, high, jnp.where(which_row == 1, mid, jnp.where(which_row == 2, low, 0.0))
    )
    upto = lax.broadcasted_iota(jnp.int32, (length, length), 0) <= lax.broadcasted_iota(
        jnp.int32, (length, length), 1
    )
    sums = dot(thirds.astype(BF16), upto.astype(F32).astype(BF16))
    cum_ref[...] = sums[0:1, :] + sums[1:2, :] + sums[2:3, :]
    a_ref[...] = in_ref[...] - cum_ref[...]

    loads[4].wait()
    loads[5].wait()
    decay = cum_ref[0:1, length - 1 : length]
    log_in = a_ref[0:1, :]
    local_top = jnp.max(log_in, axis=1, keepdims=True)
    weighted = k_ref[...].astype(F32) * jnp.exp(upright(log_in) - local_top)
    loc[HEAD : HEAD + qk, :] = dot(weighted.astype(BF16), v_ref[...], ((0,), (0,)))
    loc[0:HEAD, 0:qk] = jnp.broadcast_to(jnp.sum(weighted, axis=0, keepdims=True), (HEAD, qk))
    loc[0:HEAD, qk:vw] = jnp.broadcast_to(local_top + decay, (HEAD, vw - qk))
    loc[HEAD + qk :, :] = jnp.broadcast_to(decay, (8, vw))

    pair = pltpu.make_async_remote_copy(
        loc, pair_in, pair_send.at[0], pair_recv.at[0], device_id={"ep": flip(me, 1)}
    )

    @pl.when(core == 0)
    def _():
        pair.start()

    def gates(first_max, second_max):
        top = jnp.maximum(first_max, second_max)
        return top, jnp.exp(first_max - top), jnp.exp(second_max - top)

    def merge(target, first, second):
        second_decay = second[HEAD + qk : HEAD + qk + 1, 0:1]
        top, keep, add = gates(
            first[0:1, qk : qk + 1] + second_decay, second[0:1, qk : qk + 1]
        )
        target[0:HEAD, 0:qk] = keep * first[0:HEAD, 0:qk] + add * second[0:HEAD, 0:qk]
        target[0:HEAD, qk:vw] = jnp.broadcast_to(top, (HEAD, vw - qk))
        target[HEAD : HEAD + qk, :] = (
            keep * first[HEAD : HEAD + qk, :] + add * second[HEAD : HEAD + qk, :]
        )
        target[HEAD + qk :, :] = first[HEAD + qk :, :] + second[HEAD + qk :, :]


    def encode(target, source):
        line = lax.broadcasted_iota(jnp.int32, (LABEL, vw), 0)
        label = jnp.zeros((LABEL, vw), F32)
        for base, rest in ((0, source[0:1, :]), (3, source[HEAD + qk : HEAD + qk + 1, :])):
            for at in range(3):
                part = rest.astype(BF16).astype(F32)
                label = jnp.where(line == base + at, part, label)
                rest = rest - part
        target[0:LABEL, :] = label.astype(BF16)
        target[LABEL:, :] = source[HEAD : HEAD + qk, :].astype(BF16)

    def decode(target, source):
        label = source[0:LABEL, :].astype(F32)
        target[0:HEAD, :] = jnp.broadcast_to(label[0:1, :] + label[1:2, :] + label[2:3, :], (HEAD, vw))
        target[HEAD + qk :, :] = jnp.broadcast_to(
            label[3:4, :] + label[4:5, :] + label[5:6, :], (8, vw)
        )
        target[HEAD : HEAD + qk, :] = source[LABEL:, :].astype(F32)

    def near(ahead):
        return pltpu.make_async_remote_copy(
            near_out,
            near_in.at[ahead - 1],
            near_send.at[ahead - 1],
            near_recv.at[ahead - 1],
            device_id={"ep": me + 2 * ahead},
        )

    def carry(ahead):
        return pltpu.make_async_remote_copy(
            carry_out,
            carry_in,
            carry_send.at[ahead - 1],
            carry_recv.at[0],
            device_id={"ep": me + 2 * ahead},
        )

    down = pltpu.make_async_remote_copy(
        other, down_in, down_send.at[0], down_recv.at[0], device_id={"ep": flip(me, 1)}
    )

    @pl.when(core == 1)
    def _():
        pair.wait_recv()
        merge(both, pair_in, loc)
        encode(near_out, both)
        for ahead in range(BLOCK - 1, 0, -1):

            @pl.when(place_in_block + ahead < BLOCK)
            def _():
                near(ahead).start()

    for i in range(1, ep):

        @pl.when(held(i))
        def _():
            dispatch(i).start()

    def gather_block():
        earlier[0:HEAD, 0:qk] = jnp.zeros((HEAD, qk), F32)
        earlier[0:HEAD, qk:vw] = jnp.full((HEAD, vw - qk), LOG_FLOOR, F32)
        earlier[HEAD:, :] = jnp.zeros((qk + 8, vw), F32)
        for ahead in range(BLOCK - 1, 0, -1):

            @pl.when(place_in_block >= ahead)
            def _():
                near(ahead).wait_recv()
                decode(other, near_in.at[ahead - 1])
                merge(earlier, earlier, other)

    sends_carry = (core == 1) & (place_in_block == BLOCK - 1) & (block < last_block)

    def take_carry():
        carry(1).wait_recv()
        decode(other, carry_in)

    def send_carry(number):
        @pl.when(sends_carry & (block == number))
        def _():
            with jax.named_scope("carry"):
                if number > 0:
                    take_carry()
                    merge(other, other, earlier)
                    merge(prior, other, both)
                else:
                    merge(prior, earlier, both)
                encode(carry_out, prior)
                for ahead in range(BLOCK, 0, -1):
                    carry(ahead).start()

    with jax.named_scope("inblock"):
        loads[6].wait()
    tile = length // 4
    scale = qk**-0.5
    for at in range(4):
        rows = pl.ds(at * tile, tile)
        seen = (at + 1) * tile
        causal = lax.broadcasted_iota(jnp.int32, (tile, seen), 1) <= at * tile + (
            lax.broadcasted_iota(jnp.int32, (tile, seen), 0)
        )
        log_seen = jnp.where(causal, a_ref[0:1, 0:seen], -jnp.inf)
        top = jnp.max(log_seen, axis=1, keepdims=True)
        scores = dot(q_ref[rows, :], k_ref[0:seen, :], ((1,), (1,))) * scale
        scores = scores * jnp.exp(log_seen - top)
        num_ref[rows, :] = dot(scores.astype(BF16), v_ref[0:seen, :])
        den_ref[rows, :] = jnp.broadcast_to(jnp.sum(scores, axis=1, keepdims=True), (tile, 128))
        top_ref[rows, :] = jnp.broadcast_to(top, (tile, 128))

    loads[7].wait()
    nothing = jnp.zeros((units, width), BF16)
    for turned in range(2):
        for at in range(tp):
            unit = (at % SIDE) * SIDE + at // SIDE if turned else at
            kept = wd_ref[unit * units : (unit + 1) * units, :]
            first = at * 2 * units
            w2[turned, first : first + units, 0:width] = kept
            w2[turned, first : first + units, width : 2 * width] = nothing
            w2[turned, first + units : first + 2 * units, 0:width] = nothing
            w2[turned, first + units : first + 2 * units, width : 2 * width] = kept
    loads[8].wait()

    def turn_block(at, carry):
        source = pl.multiple_of(((at % SIDE) * SIDE + at // SIDE) * width, width)
        target = pl.multiple_of(at * width, width)
        wm_turned[pl.ds(target, width), :] = wm_ref[pl.ds(source, width), :]
        return carry

    lax.fori_loop(0, tp, turn_block, 0)

    @pl.when(core == 1)
    def _():
        with jax.named_scope("near"):
            gather_block()

    send_carry(0)


    def spread(group, k):
        rows = pl.ds(group * span, span)
        return pltpu.make_async_remote_copy(
            tok.at[rows, pl.ds(0, width)],
            tok.at[rows, pl.ds(k * width, width)],
            tok_send.at[0],
            tok_recv.at[group, k],
            device_id={"tp": flip(mine, SIDE * k)},
        )

    def onward(group, k):
        rows = pl.ds(group * span + (k // 2) * half_span, half_span)
        return pltpu.make_async_remote_copy(
            tok.at[rows, pl.ds(k * width, width)],
            tok.at[rows, pl.ds(2 * width, width)],
            tok_send.at[0],
            tok_recv.at[group, 4 + k],
            device_id={"tp": flip(mine, SIDE * (SIDE - k))},
        )

    def send_partial(group, j):
        rows = pl.ds(group * span, span)
        return pltpu.make_async_remote_copy(
            part_out.at[j, rows],
            part_in.at[j, rows],
            part_send.at[0],
            part_recv.at[group],
            device_id={"tp": flip(mine, j)},
        )

    def send_squares(group, j):
        return pltpu.make_async_remote_copy(
            sq_out.at[group],
            sq_in.at[group, j],
            sq_send.at[0],
            sq_recv.at[group],
            device_id={"tp": flip(mine, j)},
        )

    def partials(group):
        rows = pl.ds(group * span, span)
        return pltpu.make_async_remote_copy(
            part_out.at[pl.ds(1, SIDE - 1), rows],
            part_in.at[pl.ds(1, SIDE - 1), rows],
            part_send.at[0],
            part_recv.at[group],
            device_id={"tp": flip(mine, 1)},
        )

    def squares_of(group):
        foreign = sq_in.at[group, pl.ds(1, SIDE - 1)]
        return pltpu.make_async_remote_copy(
            foreign, foreign, sq_send.at[0], sq_recv.at[group], device_id={"tp": flip(mine, 1)}
        )


    def gather_copies(buffer, first_row, rows, wide_block, x_first, send, recv):
        inner, outer = (column, row) if x_first else (row, column)
        inner_bits, outer_bits = (1, SIDE) if x_first else (SIDE, 1)
        base = outer * SIDE * wide_block
        half = rows // 2

        def cut(part, block, count):
            begin, extent = (first_row, rows) if part is None else (first_row + part * half, half)
            return buffer.at[
                pl.ds(begin, extent),
                pl.ds(pl.multiple_of(base + block * wide_block, wide_block), count * wide_block),
            ]

        def outer_cut(part, bits):
            begin, extent = (first_row, rows) if part is None else (first_row + part * half, half)
            start = pl.multiple_of(flip(outer, bits) * SIDE * wide_block, SIDE * wide_block)
            return buffer.at[pl.ds(begin, extent), pl.ds(start, SIDE * wide_block)]

        def remote(piece_of, at, bits):
            return pltpu.make_async_remote_copy(
                piece_of, piece_of, send, recv.at[at], device_id={"tp": flip(mine, bits)}
            )

        def inner_send(k):
            return remote(cut(None, inner, 1), k // 2, k * inner_bits)

        def inner_relay(k):
            return remote(
                cut(k // 2, flip(inner, k), 1), 2 + k // 2, (SIDE - k) * inner_bits
            )

        def outer_send(k):
            return remote(outer_cut(None, 0), 4 + k // 2, k * outer_bits)

        def outer_relay(k):
            return remote(outer_cut(k // 2, k), 6 + k // 2, (SIDE - k) * outer_bits)

        return [[make(k) for k in (1, 3)] for make in (inner_send, inner_relay, outer_send, outer_relay)]

    def gather_step(copies, step):
        if step > 0:
            for copy in copies[step - 1]:
                copy.wait_recv()
        if step < 4:
            for copy in copies[step]:
                copy.start()

    hid_copies = [
        gather_copies(
            hid,
            group * half_span,
            half_span,
            2 * units,
            group % 2 == 0,
            hid_send.at[0],
            hid_recv.at[group],
        )
        for group in range(GROUPS)
    ]

    def give_back(i):
        return pltpu.make_async_remote_copy(
            outb.at[pl.ds(i * cap, cap)],
            ret.at[pl.ds(i * cap, cap)],
            ret_send.at[0],
            ret_recv.at[i // per],
            device_id={"ep": flip(me, i)},
        )

    def given_back(group):
        begin = cap if group == 0 else group * span
        rows = pl.ds(begin, (group + 1) * span - begin)
        return pltpu.make_async_remote_copy(
            outb.at[rows], ret.at[rows], ret_send.at[0], ret_recv.at[group], device_id={"ep": flip(me, 1)}
        )

    def stage(group, step):
        rows = pl.ds(group * span, span)
        packed = pl.ds(group * half_span, half_span)
        if step == 0:
            dispatched(group).wait_recv()
            for k in (1, 3):
                spread(group, k).start()
        elif step == 1:
            for k in (1, 3):
                spread(group, k).wait_recv()
                onward(group, k).start()
        elif step == 2:
            if group == 0:
                for load in own_pieces:
                    load.wait()
                deals().wait_recv()
            for k in (1, 3):
                onward(group, k).wait_recv()
            piece_of = tok[rows, :]
            partial = dot(piece_of, w1[...], ((1,), (1,)))
            part_own[rows, :] = partial[:, 0 : 2 * units]
            for j in range(1, SIDE):
                part_out[j, rows, :] = partial[:, j * 2 * units : (j + 1) * 2 * units].astype(BF16)
            for j in range(1, SIDE):
                send_partial(group, j).start()
            full = piece_of.astype(F32)
            squares = flat(jnp.sum(full * full, axis=1, keepdims=True))
            sq_out[group] = jnp.broadcast_to(squares, (8, span))
            for j in range(1, SIDE):
                send_squares(group, j).start()
        elif step == 3:
            squares = sq_out[group][0:1, :]
            squares_of(group).wait_recv()
            for j in range(1, SIDE):
                squares = squares + sq_in[group, j][0:1, :]
            inverse = upright(lax.rsqrt(squares / model_width + EPSILON))
            total = part_own[rows, :]
            partials(group).wait_recv()
            for j in range(1, SIDE):
                total = total + part_in[j, rows, :].astype(F32)
            total = total * inverse
            hidden = jax.nn.silu(total) * pltpu.roll(total, units, 1)
            turned = pltpu.roll(hidden, units, 1)
            lanes = lax.broadcasted_iota(jnp.int32, (half_span, 2 * units), 1)
            both_rows = jnp.where(lanes < units, hidden[0:half_span, :], turned[half_span:span, :])
            place = mine if group % 2 == 0 else column * SIDE + row
            columns = pl.ds(pl.multiple_of(place * 2 * units, 2 * units), 2 * units)
            hid[packed, columns] = both_rows.astype(BF16)
            gather_step(hid_copies[group], 0)
        elif step < 7:
            gather_step(hid_copies[group], step - 3)
        else:
            gather_step(hid_copies[group], 4)
            total = dot(hid[packed, :], w2[group % 2])
            outb[pl.ds(group * span, half_span), :] = total[:, 0:width].astype(BF16)
            outb[pl.ds(group * span + half_span, half_span), :] = total[:, width:].astype(BF16)
            for i in range(max(1, group * per), (group + 1) * per):
                give_back(i).start()

    part_rows = length // (2 * PARTS)
    head_copies = [
        gather_copies(
            hm.at[at // PARTS],
            (at % PARTS) * part_rows,
            part_rows,
            width,
            at // PARTS == 0,
            head_send.at[0],
            head_recv.at[at],
        )
        for at in range(2 * PARTS)
    ]
    orders = [at // 2 + (at % 2) * PARTS for at in range(2 * PARTS)]


    def take_prior():
        @pl.when(core == 1)
        def _():
            @pl.when((block > 0) & jnp.logical_not(sends_carry))
            def _():
                take_carry()
                merge(other, other, earlier)

            @pl.when(block == 0)
            def _():
                other[...] = earlier[...]

            down.start()
            merge(prior, other, pair_in)

        @pl.when(core == 0)
        def _():
            down.wait_recv()
            prior[...] = down_in[...]

        for load in loads[9:11]:
            load.wait()

    def finish_heads():
        prior_max = prior[0:1, qk : qk + 1]
        normal = prior[0:1, 0:qk]
        memory = prior[HEAD : HEAD + qk, :]
        high = memory.astype(BF16)
        low = (memory - high.astype(F32)).astype(BF16)
        for at in orders:
            rows = pl.ds(at * part_rows, part_rows)
            queries = q_ref[rows, :]
            own_top = top_ref[rows, 0:1]
            top = jnp.maximum(prior_max, own_top)
            again = jnp.exp(own_top - top)
            carried = jnp.exp(prior_max - top) * scale
            numerator = carried * (dot(queries, high) + dot(queries, low)) + again * num_ref[rows, :]
            denominator = (
                carried * jnp.sum(queries.astype(F32) * normal, axis=1, keepdims=True)
                + again * den_ref[rows, 0:1]
            )
            cumulative = upright(cum_ref[0:1, at * part_rows : (at + 1) * part_rows])
            floor = jnp.exp(-(cumulative + top))
            value = numerator / jnp.maximum(jnp.abs(denominator), floor)
            value = value * lax.rsqrt(jnp.mean(value * value, axis=1, keepdims=True) + EPSILON)
            gate = jax.nn.sigmoid(og_ref[rows, :].astype(F32))
            place = mine if at < PARTS else column * SIDE + row
            hm[
                at // PARTS,
                pl.ds((at % PARTS) * part_rows, part_rows),
                pl.ds(pl.multiple_of(place * width, width), width),
            ] = (value * gain_ref[...] * gate).astype(BF16)
            gather_step(head_copies[at], 0)

    def head_step(step):
        for at in orders:
            gather_step(head_copies[at], step)
            if step == 4:
                inputs = hm[at // PARTS, pl.ds((at % PARTS) * part_rows, part_rows), :]
                weights = wm_ref if at < PARTS else wm_turned
                mix_ref[pl.ds(at * part_rows, part_rows), :] = dot(inputs, weights[...]).astype(BF16)

    ticks = GROUPS + 7
    for tick in range(ticks):
        if tick == FINISH:
            with jax.named_scope("prior"):
                take_prior()
            with jax.named_scope("heads"):
                finish_heads()
        for group in range(GROUPS):
            if 0 <= tick - group < 8:
                with jax.named_scope(f"stage{group}_{tick - group}"):
                    stage(group, tick - group)
            if tick == 1 and group < 2:
                send_carry(group + 1)
        if FINISH < tick < FINISH + 5:
            with jax.named_scope(f"gather{tick - FINISH}"):
                head_step(tick - FINISH)
    ret[0:cap, :] = outb[0:cap, :]

    total = jnp.zeros((tokens, width), F32)
    places = lax.broadcasted_iota(jnp.int32, (span, tokens), 0)
    loads[11].wait()
    weights = [upright(weight_ref[route : route + 1, :]) for route in range(weight_ref.shape[0])]
    for group in range(GROUPS):
        with jax.named_scope(f"back{group}"):
            given_back(group).wait_recv()
        rows = pl.ds(group * span, span)
        for route, weight in enumerate(weights):
            hit = places == slot_row_ref[route : route + 1, :] - group * span
            picked = dot(hit.astype(F32).astype(BF16), ret[rows, :], ((0,), (0,)))
            total += picked * weight
    exp_ref[...] = total.astype(BF16)

    def sent(source, semaphore):
        pltpu.make_async_remote_copy(
            source, source, semaphore, semaphore, device_id={"ep": flip(me, 1)}
        ).wait_send()

    with jax.named_scope("drain"):
        foreign = pl.ds(cap, slots.shape[0] - cap)
        sent(slots.at[foreign], disp_send.at[0])
        sent(outb.at[foreign], ret_send.at[0])
        deals().wait_send()
        sent(tok.at[:, pl.ds(0, 3 * width)], tok_send.at[0])
        sent(part_out.at[pl.ds(1, SIDE - 1)], part_send.at[0])
        sent(sq_in.at[:, pl.ds(1, SIDE - 1)], sq_send.at[0])
        sent(hid.at[:, pl.ds(0, (tp - 1) * 2 * units)], hid_send.at[0])
        for part in range(2):
            sent(hm.at[part, :, pl.ds(0, (tp - 1) * width)], head_send.at[0])

    @pl.when(core == 0)
    def _():
        pair.wait_send()

    @pl.when(core == 1)
    def _():
        down.wait_send()
        for ahead in range(1, BLOCK):

            @pl.when(place_in_block + ahead < BLOCK)
            def _():
                near(ahead).wait_send()

    @pl.when(sends_carry)
    def _():
        for ahead in range(1, BLOCK + 1):
            carry(ahead).wait_send()


def body(
    query_rows,
    key_rows,
    value_rows,
    in_gate,
    forget_gate,
    out_gate,
    head_gain,
    mix_weight,
    expert_input,
    routes,
    route_weight,
    gate_weight,
    up_weight,
    down_weight,
):
    ep, tp = lax.axis_size("ep"), lax.axis_size("tp")
    length = in_gate.shape[1]
    token_count, fanout = routes.shape
    width = expert_input.shape[1]
    units = gate_weight.shape[1]
    capacity = 2 * token_count * fanout // ep
    slot_count = ep * capacity
    qk = query_rows.shape[1]
    vw = value_rows.shape[1]

    vmem = pl.BlockSpec(memory_space=pltpu.VMEM)
    anywhere = pl.BlockSpec(memory_space=pl.ANY)
    dma = pltpu.SemaphoreType.DMA
    gate_local, up_local, down_local = gate_weight[0], up_weight[0], down_weight[0]
    small = (expert_input, routes.T, route_weight.T, in_gate, forget_gate, head_gain[None, :])
    big = (query_rows, key_rows, value_rows, out_gate, gate_local, up_local, down_local, mix_weight)
    held = (query_rows, key_rows, value_rows, out_gate, down_local, mix_weight)
    tall = (HEAD + qk + 8, vw)
    message = (LABEL + qk, vw)
    return pl.pallas_call(
        functools.partial(kernel, ep, tp, mix_weight.shape[0]),
        out_shape=(
            jax.ShapeDtypeStruct((length, width), BF16),
            jax.ShapeDtypeStruct((token_count, width), BF16),
        ),
        in_specs=[anywhere] * 14,
        out_specs=(vmem, vmem),
        scratch_shapes=[pltpu.VMEM(array.shape, array.dtype) for array in small + held]
        + [
            pltpu.VMEM((fanout, token_count), jnp.int32),
            pltpu.VMEM((1, length), F32),
            pltpu.VMEM((1, length), F32),
            pltpu.VMEM(mix_weight.shape, BF16),
            pltpu.VMEM((SIDE * 2 * units, SIDE * width), BF16),
            pltpu.VMEM((2, tp * 2 * units, 2 * width), BF16),
            pltpu.VMEM((slot_count, width), BF16),
            pltpu.VMEM((slot_count, SIDE * width), BF16),
            pltpu.VMEM((slot_count, 2 * units), F32),
            pltpu.VMEM((SIDE, slot_count, 2 * units), BF16),
            pltpu.VMEM((SIDE, slot_count, 2 * units), BF16),
            pltpu.VMEM((GROUPS, 8, slot_count // GROUPS), F32),
            pltpu.VMEM((GROUPS, SIDE, 8, slot_count // GROUPS), F32),
            pltpu.VMEM((slot_count // 2, tp * 2 * units), BF16),
            pltpu.VMEM((slot_count, width), BF16),
            pltpu.VMEM((slot_count, width), BF16),
            pltpu.VMEM((2, length // 2, tp * width), BF16),
            pltpu.VMEM((length, vw), F32),
            pltpu.VMEM((length, 128), F32),
            pltpu.VMEM((length, 128), F32),
            pltpu.VMEM(tall, F32),
            pltpu.VMEM(tall, F32),
            pltpu.VMEM(tall, F32),
            pltpu.VMEM(tall, F32),
            pltpu.VMEM(tall, F32),
            pltpu.VMEM(tall, F32),
            pltpu.VMEM(tall, F32),
            pltpu.VMEM(message, BF16),
            pltpu.VMEM((BLOCK - 1, *message), BF16),
            pltpu.VMEM(message, BF16),
            pltpu.VMEM(message, BF16),
            dma((12,)),
            dma((2 * SIDE,)),
            dma((1,)),
            dma((1,)),
            dma((1,)),
            dma((GROUPS,)),
            dma((1,)),
            dma((GROUPS, 8)),
            dma((1,)),
            dma((GROUPS,)),
            dma((1,)),
            dma((GROUPS,)),
            dma((1,)),
            dma((GROUPS, 8)),
            dma((1,)),
            dma((GROUPS,)),
            dma((1,)),
            dma((2 * PARTS, 8)),
            dma((1,)),
            dma((1,)),
            dma((1,)),
            dma((1,)),
            dma((BLOCK - 1,)),
            dma((BLOCK - 1,)),
            dma((BLOCK,)),
            dma((1,)),
        ],
        compiler_params=pltpu.CompilerParams(
            collective_id=0, has_side_effects=True, vmem_limit_bytes=64000 * 1024
        ),
    )(*small, *big)


def solution(mesh):
    in_specs = (
        P("ep", "tp"),
        P("ep", "tp"),
        P("ep", "tp"),
        P("tp", "ep"),
        P("tp", "ep"),
        P("ep", "tp"),
        P("tp"),
        P(None, "tp"),
        P("ep", "tp"),
        P("ep", None),
        P("ep", None),
        P("ep", "tp", None),
        P("ep", "tp", None),
        P("ep", None, "tp"),
    )
    out_specs = (P("ep", "tp"), P("ep", "tp"))
    return jax.shard_map(body, mesh=mesh, in_specs=in_specs, out_specs=out_specs, check_vma=False)
```

```python
import functools

import jax
import jax.numpy as jnp
from jax import lax
from jax.experimental import pallas as pl
from jax.experimental.pallas import tpu as pltpu
from jax.sharding import PartitionSpec as P

EPSILON = 1e-06
LOG_FLOOR = -1e30
F32 = jnp.float32
BF16 = jnp.bfloat16
GROUPS = 4
SIDE = 4
PARTS = 4
BLOCK = 4
HEAD = 8
LABEL = 16
SEQUENCE = (
    "s00", "d0", "s01", "s10", "h0", "s02", "s20", "s11", "near", "s03", "s21", "s30", "s12",
    "carry1", "s04", "s22", "s31", "build", "s13", "s05", "carry2", "s23", "s14", "s32", "s24",
    "s06", "d1", "heads", "s15", "g0", "s33", "s25", "s16", "g1", "s34", "g2", "h1", "g3", "m0",
    "s26", "s35", "m1", "m2", "m3", "s36", "f0", "f1", "f2", "f3",
)
ORDER = (0, 3, -3, 4, 8, 7, -7, -6, 6, 5, -5, -4, 2, 1, -1, -2)


def flip(index, bits):
    place = 1
    while place <= bits:
        if bits & place:
            index = index + place * (1 - 2 * ((index // place) % 2))
        place *= 2
    return index


def dot(left, right, contract=((1,), (0,))):
    return lax.dot_general(left, right, (contract, ((), ())), preferred_element_type=F32)


def own_mask(size):
    return lax.broadcasted_iota(jnp.int32, (size, size), 0) == lax.broadcasted_iota(
        jnp.int32, (size, size), 1
    )


def upright(row):
    size = row.shape[1]
    return jnp.sum(jnp.where(own_mask(size), row, 0.0), axis=1, keepdims=True)


def flat(column):
    size = column.shape[0]
    return jnp.sum(jnp.where(own_mask(size), column, 0.0), axis=0, keepdims=True)


def kernel(
    ep,
    tp,
    model_width,
    x_hbm,
    routes_hbm,
    weight_hbm,
    in_hbm,
    forget_hbm,
    gain_hbm,
    q_hbm,
    k_hbm,
    v_hbm,
    og_hbm,
    wg_hbm,
    wu_hbm,
    wd_hbm,
    wm_hbm,
    mix_ref,
    exp_ref,
    x_ref,
    routes_ref,
    weight_ref,
    in_ref,
    forget_ref,
    gain_ref,
    q_ref,
    k_ref,
    v_ref,
    og_ref,
    wd_ref,
    slot_row_ref,
    a_ref,
    cum_ref,
    w1,
    wmix,
    w2,
    slots,
    tok,
    part_own,
    part_out,
    part_in,
    sq_out,
    sq_in,
    hid,
    outb,
    ret,
    hm,
    mix_own,
    mix_out,
    mix_in,
    num_ref,
    den_ref,
    top_ref,
    loc,
    pair_in,
    both,
    earlier,
    other,
    prior,
    down_in,
    near_out,
    near_in,
    carry_out,
    carry_in,
    load_sem,
    own_sem,
    deal_send,
    deal_recv,
    mix_deal_send,
    mix_deal_recv,
    hand_send,
    hand_recv,
    disp_send,
    disp_recv,
    tok_send,
    tok_recv,
    part_send,
    part_recv,
    sq_send,
    sq_recv,
    hid_send,
    hid_recv,
    ret_send,
    ret_recv,
    head_send,
    head_recv,
    mix_send,
    mix_recv,
    pair_send,
    pair_recv,
    down_send,
    down_recv,
    near_send,
    near_recv,
    carry_send,
    carry_recv,
):
    me = lax.axis_index("ep")
    mine = lax.axis_index("tp")
    row, column = mine // SIDE, mine % SIDE
    chip, core = me // 2, me % 2
    chips = ep // 2
    block, place_in_block = chip // BLOCK, chip % BLOCK
    last_block = chips // BLOCK - 1
    cap = slots.shape[0] // ep
    span = slots.shape[0] // GROUPS
    half_span = span // 2
    per = ep // GROUPS
    width = x_ref.shape[1]
    tokens = x_ref.shape[0]
    length, qk = q_ref.shape
    vw = v_ref.shape[1]
    units = wg_hbm.shape[0]
    wide = SIDE * width

    names = (
        (routes_hbm, routes_ref),
        (x_hbm, x_ref),
        (forget_hbm, forget_ref),
        (in_hbm, in_ref),
        (k_hbm, k_ref),
        (v_hbm, v_ref),
        (q_hbm, q_ref),
        (wd_hbm, wd_ref),
        (og_hbm, og_ref),
        (gain_hbm, gain_ref),
        (weight_hbm, weight_ref),
    )
    loads = [
        pltpu.make_async_copy(source, target, load_sem.at[at])
        for at, (source, target) in enumerate(names)
    ]
    for load in loads:
        load.start()

    def piece(source, j, k):
        start = pl.multiple_of((flip(row, k) * SIDE + flip(column, j)) * width, width)
        return source.at[:, pl.ds(start, width)]

    def slot_of(j, which, k):
        return w1.at[pl.ds((2 * j + which) * units, units), pl.ds(k * width, width)]

    own_pieces = [
        pltpu.make_async_copy(
            piece(source, 0, k), slot_of(0, which, k), own_sem.at[which * SIDE + k]
        )
        for which, source in enumerate((wg_hbm, wu_hbm))
        for k in range(SIDE)
    ]

    def mix_piece(j, k):
        turned = row + (k % 2) * (1 - 2 * (row % 2)) + 2 * (k // 2) * (1 - 2 * (row // 2 % 2))
        start = pl.multiple_of((turned * SIDE + flip(column, j)) * width, width)
        return wm_hbm.at[pl.ds(start, width), :]

    def mix_slot(j, k):
        return wmix.at[pl.ds(pl.multiple_of(k * width, width), width), pl.ds(j * width, width)]

    own_pieces += [
        pltpu.make_async_copy(mix_piece(0, k), mix_slot(0, k), own_sem.at[2 * SIDE + k])
        for k in range(SIDE)
    ]
    for load in own_pieces:
        load.start()


    def deal_mix(j, at):
        k = core + 2 * at
        return pltpu.make_async_remote_copy(
            mix_piece(j, k),
            mix_slot(j, k),
            mix_deal_send.at[0],
            mix_deal_recv.at[at],
            device_id={"tp": flip(mine, j)},
        )

    def foreign_rows(k):
        start = pl.multiple_of(k * width, width)
        return wmix.at[pl.ds(start, width), pl.ds(width, (SIDE - 1) * width)]

    def mix_dealt(at):
        foreign = foreign_rows(core + 2 * at)
        return pltpu.make_async_remote_copy(
            foreign, foreign, mix_deal_send.at[0], mix_deal_recv.at[at], device_id={"tp": flip(mine, 1)}
        )

    def hand_mix(at, whose):
        foreign = foreign_rows(whose + 2 * at)
        return pltpu.make_async_remote_copy(
            foreign, foreign, hand_send.at[at], hand_recv.at[at], device_id={"ep": flip(me, 1)}
        )

    def deal(j, which, k):
        return pltpu.make_async_remote_copy(
            piece(wu_hbm if which else wg_hbm, j, k),
            slot_of(j, which, k),
            deal_send.at[0],
            deal_recv.at[0],
            device_id={"tp": flip(mine, j)},
        )

    def deals():
        foreign = w1.at[pl.ds(2 * units, 2 * (SIDE - 1) * units)]
        return pltpu.make_async_remote_copy(
            foreign, foreign, deal_send.at[0], deal_recv.at[0], device_id={"tp": flip(mine, 1)}
        )

    dealt = [(j, which, k) for j in range(1, SIDE) for which in range(2) for k in range(SIDE)]

    barrier = pltpu.get_barrier_semaphore()
    for i in range(1, ep):
        pl.semaphore_signal(barrier, inc=1, device_id={"ep": flip(me, i)})
    for j in range(1, tp):
        pl.semaphore_signal(barrier, inc=1, device_id={"tp": flip(mine, j)})

    loads[0].wait()
    experts = lax.broadcasted_iota(jnp.int32, (ep, tokens), 0)

    offsets = ORDER if chips == len(ORDER) else tuple(range(chips))

    def turn_of(expert):
        ahead = ((expert >> 1) - chip) & (chips - 1)
        step = jnp.zeros_like(ahead)
        for at, ahead_of in enumerate(offsets):
            step = jnp.where(ahead == ahead_of % chips, at, step)
        return 2 * step + ((expert & 1) ^ core)

    named = [experts == turn_of(routes_ref[route : route + 1, :]) for route in range(2)]
    any_named = (named[0] | named[1]).astype(F32).astype(BF16)
    older = lax.broadcasted_iota(jnp.int32, (tokens, tokens), 0) < lax.broadcasted_iota(
        jnp.int32, (tokens, tokens), 1
    )
    before = dot(any_named, older.astype(F32).astype(BF16))
    places = (experts * cap).astype(F32) + before
    for route in range(2):
        slot_row_ref[route : route + 1, :] = jnp.sum(
            jnp.where(named[route], places, 0.0), axis=0, keepdims=True
        ).astype(jnp.int32)
    loads[1].wait()

    def pick(group, carry):
        at = group * span
        rows = at + lax.broadcasted_iota(jnp.int32, (span, tokens), 0)
        hit = (rows == slot_row_ref[0:1, :]) | (rows == slot_row_ref[1:2, :])
        chosen = dot(hit.astype(F32).astype(BF16), x_ref[...]).astype(BF16)
        slots[pl.ds(pl.multiple_of(at, span), span), :] = chosen
        return carry

    lax.fori_loop(0, GROUPS, pick, 0)

    with jax.named_scope("barrier"):
        pl.semaphore_wait(barrier, ep - 1 + tp - 1)

    def peer(i, sign):
        return 2 * ((chip + sign * offsets[i // 2] + chips) % chips) + (core + i) % 2

    def dispatch(i):
        return pltpu.make_async_remote_copy(
            slots.at[pl.ds(i * cap, cap)],
            tok.at[pl.ds(i * cap, cap), pl.ds(0, width)],
            disp_send.at[0],
            disp_recv.at[i // per],
            device_id={"ep": peer(i, 1)},
        )

    def dispatched(group):
        begin = cap if group == 0 else group * span
        rows = pl.ds(begin, (group + 1) * span - begin)
        return pltpu.make_async_remote_copy(
            slots.at[rows],
            tok.at[rows, pl.ds(0, width)],
            disp_send.at[0],
            disp_recv.at[group],
            device_id={"ep": flip(me, 1)},
        )

    for i in range(1, ep):
        dispatch(i).start()

    tok[0:cap, 0:width] = slots[0:cap, :]
    for each in dealt:
        deal(*each).start()


    loads[2].wait()
    loads[3].wait()
    gates_in = forget_ref[...]
    log_keep = jnp.minimum(gates_in, 0.0) - jnp.log1p(jnp.exp(-jnp.abs(gates_in)))
    high = log_keep.astype(BF16).astype(F32)
    mid = (log_keep - high).astype(BF16).astype(F32)
    low = log_keep - high - mid
    which_row = lax.broadcasted_iota(jnp.int32, (8, length), 0)
    thirds = jnp.where(
        which_row == 0, high, jnp.where(which_row == 1, mid, jnp.where(which_row == 2, low, 0.0))
    )
    upto = lax.broadcasted_iota(jnp.int32, (length, length), 0) <= lax.broadcasted_iota(
        jnp.int32, (length, length), 1
    )
    sums = dot(thirds.astype(BF16), upto.astype(F32).astype(BF16))
    cum_ref[...] = sums[0:1, :] + sums[1:2, :] + sums[2:3, :]
    a_ref[...] = in_ref[...] - cum_ref[...]

    loads[4].wait()
    loads[5].wait()
    decay = cum_ref[0:1, length - 1 : length]
    log_in = a_ref[0:1, :]
    local_top = jnp.max(log_in, axis=1, keepdims=True)
    weighted = k_ref[...].astype(F32) * jnp.exp(upright(log_in) - local_top)
    loc[HEAD : HEAD + qk, :] = dot(weighted.astype(BF16), v_ref[...], ((0,), (0,)))
    loc[0:HEAD, 0:qk] = jnp.broadcast_to(jnp.sum(weighted, axis=0, keepdims=True), (HEAD, qk))
    loc[0:HEAD, qk:vw] = jnp.broadcast_to(local_top + decay, (HEAD, vw - qk))
    loc[HEAD + qk :, :] = jnp.broadcast_to(decay, (8, vw))

    pair = pltpu.make_async_remote_copy(
        loc, pair_in, pair_send.at[0], pair_recv.at[0], device_id={"ep": flip(me, 1)}
    )

    @pl.when(core == 0)
    def _():
        pair.start()

    def gates(first_max, second_max):
        top = jnp.maximum(first_max, second_max)
        return top, jnp.exp(first_max - top), jnp.exp(second_max - top)

    def merge(target, first, second):
        second_decay = second[HEAD + qk : HEAD + qk + 1, 0:1]
        top, keep, add = gates(
            first[0:1, qk : qk + 1] + second_decay, second[0:1, qk : qk + 1]
        )
        target[0:HEAD, 0:qk] = keep * first[0:HEAD, 0:qk] + add * second[0:HEAD, 0:qk]
        target[0:HEAD, qk:vw] = jnp.broadcast_to(top, (HEAD, vw - qk))
        target[HEAD : HEAD + qk, :] = (
            keep * first[HEAD : HEAD + qk, :] + add * second[HEAD : HEAD + qk, :]
        )
        target[HEAD + qk :, :] = first[HEAD + qk :, :] + second[HEAD + qk :, :]


    def encode(target, source):
        line = lax.broadcasted_iota(jnp.int32, (LABEL, vw), 0)
        label = jnp.zeros((LABEL, vw), F32)
        for base, rest in ((0, source[0:1, :]), (3, source[HEAD + qk : HEAD + qk + 1, :])):
            for at in range(3):
                part = rest.astype(BF16).astype(F32)
                label = jnp.where(line == base + at, part, label)
                rest = rest - part
        target[0:LABEL, :] = label.astype(BF16)
        target[LABEL:, :] = source[HEAD : HEAD + qk, :].astype(BF16)

    def decode(target, source):
        label = source[0:LABEL, :].astype(F32)
        target[0:HEAD, :] = jnp.broadcast_to(label[0:1, :] + label[1:2, :] + label[2:3, :], (HEAD, vw))
        target[HEAD + qk :, :] = jnp.broadcast_to(
            label[3:4, :] + label[4:5, :] + label[5:6, :], (8, vw)
        )
        target[HEAD : HEAD + qk, :] = source[LABEL:, :].astype(F32)

    def near(ahead):
        return pltpu.make_async_remote_copy(
            near_out,
            near_in.at[ahead - 1],
            near_send.at[ahead - 1],
            near_recv.at[ahead - 1],
            device_id={"ep": me + 2 * ahead},
        )

    def carry(ahead):
        return pltpu.make_async_remote_copy(
            carry_out,
            carry_in,
            carry_send.at[ahead - 1],
            carry_recv.at[0],
            device_id={"ep": me + 2 * ahead},
        )

    down = pltpu.make_async_remote_copy(
        other, down_in, down_send.at[0], down_recv.at[0], device_id={"ep": flip(me, 1)}
    )

    @pl.when(core == 1)
    def _():
        pair.wait_recv()
        merge(both, pair_in, loc)
        encode(near_out, both)
        for ahead in range(BLOCK - 1, 0, -1):

            @pl.when(place_in_block + ahead < BLOCK)
            def _():
                near(ahead).start()

    def gather_block():
        earlier[0:HEAD, 0:qk] = jnp.zeros((HEAD, qk), F32)
        earlier[0:HEAD, qk:vw] = jnp.full((HEAD, vw - qk), LOG_FLOOR, F32)
        earlier[HEAD:, :] = jnp.zeros((qk + 8, vw), F32)
        for ahead in range(BLOCK - 1, 0, -1):

            @pl.when(place_in_block >= ahead)
            def _():
                near(ahead).wait_recv()
                decode(other, near_in.at[ahead - 1])
                merge(earlier, earlier, other)

    sends_carry = (core == 1) & (place_in_block == BLOCK - 1) & (block < last_block)

    def take_carry():
        carry(1).wait_recv()
        decode(other, carry_in)

    def send_carry(number):
        @pl.when(sends_carry & (block == number))
        def _():
            with jax.named_scope("carry"):
                if number > 0:
                    take_carry()
                    merge(other, other, earlier)
                    merge(prior, other, both)
                else:
                    merge(prior, earlier, both)
                encode(carry_out, prior)
                for ahead in range(BLOCK, 0, -1):
                    carry(ahead).start()

    with jax.named_scope("inblock"):
        loads[6].wait()
    tile = length // 4
    scale = qk**-0.5
    for at in range(4):
        rows = pl.ds(at * tile, tile)
        seen = (at + 1) * tile
        causal = lax.broadcasted_iota(jnp.int32, (tile, seen), 1) <= at * tile + (
            lax.broadcasted_iota(jnp.int32, (tile, seen), 0)
        )
        log_seen = jnp.where(causal, a_ref[0:1, 0:seen], -jnp.inf)
        top = jnp.max(log_seen, axis=1, keepdims=True)
        scores = dot(q_ref[rows, :], k_ref[0:seen, :], ((1,), (1,))) * scale
        scores = scores * jnp.exp(log_seen - top)
        num_ref[rows, :] = dot(scores.astype(BF16), v_ref[0:seen, :])
        den_ref[rows, :] = jnp.broadcast_to(jnp.sum(scores, axis=1, keepdims=True), (tile, 128))
        top_ref[rows, :] = jnp.broadcast_to(top, (tile, 128))


    def build_down():
        loads[7].wait()
        nothing = jnp.zeros((units, width), BF16)
        for at in range(tp):
            kept = wd_ref[at * units : (at + 1) * units, :]
            first = at * 2 * units
            w2[first : first + units, 0:width] = kept
            w2[first : first + units, width : 2 * width] = nothing
            w2[first + units : first + 2 * units, 0:width] = nothing
            w2[first + units : first + 2 * units, width : 2 * width] = kept


    def spread(group, k):
        rows = pl.ds(group * span, span)
        return pltpu.make_async_remote_copy(
            tok.at[rows, pl.ds(0, width)],
            tok.at[rows, pl.ds(k * width, width)],
            tok_send.at[0],
            tok_recv.at[group, k // 2],
            device_id={"tp": flip(mine, SIDE * k)},
        )

    def onward(group, k):
        rows = pl.ds(group * span + (k // 2) * half_span, half_span)
        return pltpu.make_async_remote_copy(
            tok.at[rows, pl.ds(k * width, width)],
            tok.at[rows, pl.ds(2 * width, width)],
            tok_send.at[0],
            tok_recv.at[group, 2 + k // 2],
            device_id={"tp": flip(mine, SIDE * (SIDE - k))},
        )

    def send_partial(group, j):
        rows = pl.ds(group * span, span)
        return pltpu.make_async_remote_copy(
            part_out.at[j, rows],
            part_in.at[j, rows],
            part_send.at[0],
            part_recv.at[group],
            device_id={"tp": flip(mine, j)},
        )

    def send_squares(group, j):
        return pltpu.make_async_remote_copy(
            sq_out.at[group],
            sq_in.at[group, j],
            sq_send.at[0],
            sq_recv.at[group],
            device_id={"tp": flip(mine, j)},
        )

    def partials(group):
        rows = pl.ds(group * span, span)
        return pltpu.make_async_remote_copy(
            part_out.at[pl.ds(1, SIDE - 1), rows],
            part_in.at[pl.ds(1, SIDE - 1), rows],
            part_send.at[0],
            part_recv.at[group],
            device_id={"tp": flip(mine, 1)},
        )

    def squares_of(group):
        foreign = sq_in.at[group, pl.ds(1, SIDE - 1)]
        return pltpu.make_async_remote_copy(
            foreign, foreign, sq_send.at[0], sq_recv.at[group], device_id={"tp": flip(mine, 1)}
        )


    def hid_block(group, at, count):
        return hid.at[
            pl.ds(group * half_span, half_span),
            pl.ds(pl.multiple_of(at * 2 * units, 2 * units), count * 2 * units),
        ]

    def hid_inner(group, k):
        block_of = hid_block(group, mine, 1)
        return pltpu.make_async_remote_copy(
            block_of, block_of, hid_send.at[0], hid_recv.at[group, 0], device_id={"tp": flip(mine, k)}
        )

    def hid_outer(group, k):
        block_of = hid_block(group, row * SIDE, SIDE)
        return pltpu.make_async_remote_copy(
            block_of,
            block_of,
            hid_send.at[0],
            hid_recv.at[group, 1 + k // 2],
            device_id={"tp": flip(mine, SIDE * k)},
        )

    def hid_onward(group, k):
        quarter = half_span // 2
        block_of = hid.at[
            pl.ds(group * half_span + (k // 2) * quarter, quarter),
            pl.ds(pl.multiple_of(flip(row, k) * SIDE * 2 * units, SIDE * 2 * units), SIDE * 2 * units),
        ]
        return pltpu.make_async_remote_copy(
            block_of,
            block_of,
            hid_send.at[0],
            hid_recv.at[group, 3 + k // 2],
            device_id={"tp": flip(mine, SIDE * (SIDE - k))},
        )

    def hid_row(group):
        foreign = hid_block(group, 0, SIDE - 1)
        return pltpu.make_async_remote_copy(
            foreign, foreign, hid_send.at[0], hid_recv.at[group, 0], device_id={"tp": flip(mine, 1)}
        )

    def give_back(i):
        return pltpu.make_async_remote_copy(
            outb.at[pl.ds(i * cap, cap)],
            ret.at[pl.ds(i * cap, cap)],
            ret_send.at[0],
            ret_recv.at[i // per],
            device_id={"ep": peer(i, -1)},
        )

    def given_back(group):
        begin = cap if group == 0 else group * span
        rows = pl.ds(begin, (group + 1) * span - begin)
        return pltpu.make_async_remote_copy(
            outb.at[rows], ret.at[rows], ret_send.at[0], ret_recv.at[group], device_id={"ep": flip(me, 1)}
        )

    def stage(group, step):
        rows = pl.ds(group * span, span)
        packed = pl.ds(group * half_span, half_span)
        if step == 0:
            dispatched(group).wait_recv()
            for k in (1, 3):
                spread(group, k).start()
        elif step == 1:
            for k in (1, 3):
                spread(group, k).wait_recv()
                onward(group, k).start()
        elif step == 2:
            if group == 0:
                for load in own_pieces[0 : 2 * SIDE]:
                    load.wait()
                deals().wait_recv()
            for k in (1, 3):
                onward(group, k).wait_recv()
            piece_of = tok[rows, :]
            partial = dot(piece_of, w1[...], ((1,), (1,)))
            part_own[rows, :] = partial[:, 0 : 2 * units]
            for j in range(1, SIDE):
                part_out[j, rows, :] = partial[:, j * 2 * units : (j + 1) * 2 * units].astype(BF16)
            for j in range(1, SIDE):
                send_partial(group, j).start()
            full = piece_of.astype(F32)
            squares = flat(jnp.sum(full * full, axis=1, keepdims=True))
            sq_out[group] = jnp.broadcast_to(squares, (8, span))
            for j in range(1, SIDE):
                send_squares(group, j).start()
        elif step == 3:
            squares = sq_out[group][0:1, :]
            squares_of(group).wait_recv()
            for j in range(1, SIDE):
                squares = squares + sq_in[group, j][0:1, :]
            inverse = upright(lax.rsqrt(squares / model_width + EPSILON))
            total = part_own[rows, :]
            partials(group).wait_recv()
            for j in range(1, SIDE):
                total = total + part_in[j, rows, :].astype(F32)
            total = total * inverse
            hidden = jax.nn.silu(total) * pltpu.roll(total, units, 1)
            turned = pltpu.roll(hidden, units, 1)
            lanes = lax.broadcasted_iota(jnp.int32, (half_span, 2 * units), 1)
            both_rows = jnp.where(lanes < units, hidden[0:half_span, :], turned[half_span:span, :])
            columns = pl.ds(pl.multiple_of(mine * 2 * units, 2 * units), 2 * units)
            hid[packed, columns] = both_rows.astype(BF16)
            for k in range(1, SIDE):
                hid_inner(group, k).start()
        elif step == 4:
            hid_row(group).wait_recv()
            for k in (1, 3):
                hid_outer(group, k).start()
        elif step == 5:
            for k in (1, 3):
                hid_outer(group, k).wait_recv()
                hid_onward(group, k).start()
        else:
            for k in (1, 3):
                hid_onward(group, k).wait_recv()
            total = dot(hid[packed, :], w2[...])
            outb[pl.ds(group * span, half_span), :] = total[:, 0:width].astype(BF16)
            outb[pl.ds(group * span + half_span, half_span), :] = total[:, width:].astype(BF16)
            for i in range(max(1, group * per), (group + 1) * per):
                give_back(i).start()

    part_rows = length // PARTS

    def head_spread(at, k):
        rows = pl.ds(at * part_rows, part_rows)
        return pltpu.make_async_remote_copy(
            hm.at[rows, pl.ds(0, width)],
            hm.at[rows, pl.ds(k * width, width)],
            head_send.at[0],
            head_recv.at[at],
            device_id={"tp": flip(mine, SIDE * k)},
        )

    def heads_of(at):
        foreign = hm.at[pl.ds(at * part_rows, part_rows), pl.ds(width, (SIDE - 1) * width)]
        return pltpu.make_async_remote_copy(
            foreign, foreign, head_send.at[0], head_recv.at[at], device_id={"tp": flip(mine, 1)}
        )

    def mix_partial(at, j):
        rows = pl.ds(at * part_rows, part_rows)
        return pltpu.make_async_remote_copy(
            mix_out.at[j, rows],
            mix_in.at[j, rows],
            mix_send.at[0],
            mix_recv.at[at],
            device_id={"tp": flip(mine, j)},
        )

    def mix_partials(at):
        foreign = mix_in.at[pl.ds(1, SIDE - 1), pl.ds(at * part_rows, part_rows)]
        return pltpu.make_async_remote_copy(
            foreign, foreign, mix_send.at[0], mix_recv.at[at], device_id={"tp": flip(mine, 1)}
        )


    def take_prior():
        @pl.when(core == 1)
        def _():
            @pl.when((block > 0) & jnp.logical_not(sends_carry))
            def _():
                take_carry()
                merge(other, other, earlier)

            @pl.when(block == 0)
            def _():
                other[...] = earlier[...]

            down.start()
            merge(prior, other, pair_in)

        @pl.when(core == 0)
        def _():
            down.wait_recv()
            prior[...] = down_in[...]

        for load in loads[8:10]:
            load.wait()

    def finish_heads(at):
        prior_max = prior[0:1, qk : qk + 1]
        normal = prior[0:1, 0:qk]
        memory = prior[HEAD : HEAD + qk, :]
        high = memory.astype(BF16)
        low = (memory - high.astype(F32)).astype(BF16)
        rows = pl.ds(at * part_rows, part_rows)
        queries = q_ref[rows, :]
        own_top = top_ref[rows, 0:1]
        top = jnp.maximum(prior_max, own_top)
        again = jnp.exp(own_top - top)
        carried = jnp.exp(prior_max - top) * scale
        numerator = carried * (dot(queries, high) + dot(queries, low)) + again * num_ref[rows, :]
        denominator = (
            carried * jnp.sum(queries.astype(F32) * normal, axis=1, keepdims=True)
            + again * den_ref[rows, 0:1]
        )
        cumulative = upright(cum_ref[0:1, at * part_rows : (at + 1) * part_rows])
        floor = jnp.exp(-(cumulative + top))
        value = numerator / jnp.maximum(jnp.abs(denominator), floor)
        value = value * lax.rsqrt(jnp.mean(value * value, axis=1, keepdims=True) + EPSILON)
        gate = jax.nn.sigmoid(og_ref[rows, :].astype(F32))
        hm[rows, 0:width] = (value * gain_ref[...] * gate).astype(BF16)
        for k in range(1, SIDE):
            head_spread(at, k).start()

    def mix_step(at):
        if at == first_mixed:
            for load in own_pieces[2 * SIDE :]:
                load.wait()
            for half in range(2):
                hand_mix(half, 1 - core).wait_recv()
        heads_of(at).wait_recv()
        rows = pl.ds(at * part_rows, part_rows)
        partial = dot(hm[rows, :], wmix[...])
        mix_own[rows, :] = partial[:, 0:width]
        for j in range(1, SIDE):
            mix_out[j, rows, :] = partial[:, j * width : (j + 1) * width].astype(BF16)
        for j in range(1, SIDE):
            mix_partial(at, j).start()

    def mix_finish(at):
        mix_partials(at).wait_recv()
        rows = pl.ds(at * part_rows, part_rows)
        total = mix_own[rows, :]
        for j in range(1, SIDE):
            total = total + mix_in[j, rows, :].astype(F32)
        mix_ref[rows, :] = total.astype(BF16)

    def near_step():
        @pl.when(core == 1)
        def _():
            gather_block()

        send_carry(0)

    first_mixed = min((SEQUENCE.index(f"m{at}"), at) for at in range(PARTS))[1]

    def deal_step(at):
        for j in range(1, SIDE):
            deal_mix(j, at).start()

    def hand_step(at):
        mix_dealt(at).wait_recv()
        hand_mix(at, core).start()

    named_steps = {
        "near": near_step,
        "heads": take_prior,
        "build": build_down,
        "carry1": lambda: send_carry(1),
        "carry2": lambda: send_carry(2),
    }
    for item in SEQUENCE:
        with jax.named_scope(item):
            if item in named_steps:
                named_steps[item]()
            elif item[0] == "s":
                stage(int(item[1]), int(item[2]))
            elif item[0] == "d":
                deal_step(int(item[1]))
            elif item[0] == "h" and item != "heads":
                hand_step(int(item[1]))
            elif item[0] == "g":
                finish_heads(int(item[1]))
            elif item[0] == "m":
                mix_step(int(item[1]))
            else:
                mix_finish(int(item[1]))
    ret[0:cap, :] = outb[0:cap, :]

    total = jnp.zeros((tokens, width), F32)
    places = lax.broadcasted_iota(jnp.int32, (span, tokens), 0)
    loads[10].wait()
    weights = [upright(weight_ref[route : route + 1, :]) for route in range(weight_ref.shape[0])]
    for group in range(GROUPS):
        with jax.named_scope(f"back{group}"):
            given_back(group).wait_recv()
        rows = pl.ds(group * span, span)
        for route, weight in enumerate(weights):
            hit = places == slot_row_ref[route : route + 1, :] - group * span
            picked = dot(hit.astype(F32).astype(BF16), ret[rows, :], ((0,), (0,)))
            total += picked * weight
    exp_ref[...] = total.astype(BF16)

    def sent(source, semaphore):
        pltpu.make_async_remote_copy(
            source, source, semaphore, semaphore, device_id={"ep": flip(me, 1)}
        ).wait_send()

    with jax.named_scope("drain"):
        foreign = pl.ds(cap, slots.shape[0] - cap)
        sent(slots.at[foreign], disp_send.at[0])
        sent(outb.at[foreign], ret_send.at[0])
        deals().wait_send()
        sent(tok.at[:, pl.ds(0, 3 * width)], tok_send.at[0])
        for half in range(2):
            mix_dealt(half).wait_send()
            hand_mix(half, core).wait_send()
        sent(part_out.at[pl.ds(1, SIDE - 1)], part_send.at[0])
        sent(sq_in.at[:, pl.ds(1, SIDE - 1)], sq_send.at[0])
        sent(hid.at[:, pl.ds(0, (tp - 1) * 2 * units)], hid_send.at[0])
        sent(hm.at[:, pl.ds(0, (SIDE - 1) * width)], head_send.at[0])
        sent(mix_in.at[pl.ds(1, SIDE - 1)], mix_send.at[0])

    @pl.when(core == 0)
    def _():
        pair.wait_send()

    @pl.when(core == 1)
    def _():
        down.wait_send()
        for ahead in range(1, BLOCK):

            @pl.when(place_in_block + ahead < BLOCK)
            def _():
                near(ahead).wait_send()

    @pl.when(sends_carry)
    def _():
        for ahead in range(1, BLOCK + 1):
            carry(ahead).wait_send()


def body(
    query_rows,
    key_rows,
    value_rows,
    in_gate,
    forget_gate,
    out_gate,
    head_gain,
    mix_weight,
    expert_input,
    routes,
    route_weight,
    gate_weight,
    up_weight,
    down_weight,
):
    ep, tp = lax.axis_size("ep"), lax.axis_size("tp")
    length = in_gate.shape[1]
    token_count, fanout = routes.shape
    width = expert_input.shape[1]
    units = gate_weight.shape[1]
    capacity = 2 * token_count * fanout // ep
    slot_count = ep * capacity
    qk = query_rows.shape[1]
    vw = value_rows.shape[1]

    vmem = pl.BlockSpec(memory_space=pltpu.VMEM)
    anywhere = pl.BlockSpec(memory_space=pl.ANY)
    dma = pltpu.SemaphoreType.DMA
    gate_local, up_local, down_local = gate_weight[0], up_weight[0], down_weight[0]
    small = (expert_input, routes.T, route_weight.T, in_gate, forget_gate, head_gain[None, :])
    big = (query_rows, key_rows, value_rows, out_gate, gate_local, up_local, down_local, mix_weight)
    held = (query_rows, key_rows, value_rows, out_gate, down_local)
    tall = (HEAD + qk + 8, vw)
    message = (LABEL + qk, vw)
    return pl.pallas_call(
        functools.partial(kernel, ep, tp, mix_weight.shape[0]),
        out_shape=(
            jax.ShapeDtypeStruct((length, width), BF16),
            jax.ShapeDtypeStruct((token_count, width), BF16),
        ),
        in_specs=[anywhere] * 14,
        out_specs=(vmem, vmem),
        scratch_shapes=[pltpu.VMEM(array.shape, array.dtype) for array in small + held]
        + [
            pltpu.VMEM((fanout, token_count), jnp.int32),
            pltpu.VMEM((1, length), F32),
            pltpu.VMEM((1, length), F32),
            pltpu.VMEM((SIDE * 2 * units, SIDE * width), BF16),
            pltpu.VMEM((SIDE * width, SIDE * width), BF16),
            pltpu.VMEM((tp * 2 * units, 2 * width), BF16),
            pltpu.VMEM((slot_count, width), BF16),
            pltpu.VMEM((slot_count, SIDE * width), BF16),
            pltpu.VMEM((slot_count, 2 * units), F32),
            pltpu.VMEM((SIDE, slot_count, 2 * units), BF16),
            pltpu.VMEM((SIDE, slot_count, 2 * units), BF16),
            pltpu.VMEM((GROUPS, 8, slot_count // GROUPS), F32),
            pltpu.VMEM((GROUPS, SIDE, 8, slot_count // GROUPS), F32),
            pltpu.VMEM((slot_count // 2, tp * 2 * units), BF16),
            pltpu.VMEM((slot_count, width), BF16),
            pltpu.VMEM((slot_count, width), BF16),
            pltpu.VMEM((length, SIDE * width), BF16),
            pltpu.VMEM((length, width), F32),
            pltpu.VMEM((SIDE, length, width), BF16),
            pltpu.VMEM((SIDE, length, width), BF16),
            pltpu.VMEM((length, vw), F32),
            pltpu.VMEM((length, 128), F32),
            pltpu.VMEM((length, 128), F32),
            pltpu.VMEM(tall, F32),
            pltpu.VMEM(tall, F32),
            pltpu.VMEM(tall, F32),
            pltpu.VMEM(tall, F32),
            pltpu.VMEM(tall, F32),
            pltpu.VMEM(tall, F32),
            pltpu.VMEM(tall, F32),
            pltpu.VMEM(message, BF16),
            pltpu.VMEM((BLOCK - 1, *message), BF16),
            pltpu.VMEM(message, BF16),
            pltpu.VMEM(message, BF16),
            dma((11,)),
            dma((3 * SIDE,)),
            dma((1,)),
            dma((1,)),
            dma((1,)),
            dma((2,)),
            dma((2,)),
            dma((2,)),
            dma((1,)),
            dma((GROUPS,)),
            dma((1,)),
            dma((GROUPS, 4)),
            dma((1,)),
            dma((GROUPS,)),
            dma((1,)),
            dma((GROUPS,)),
            dma((1,)),
            dma((GROUPS, 5)),
            dma((1,)),
            dma((GROUPS,)),
            dma((1,)),
            dma((PARTS,)),
            dma((1,)),
            dma((PARTS,)),
            dma((1,)),
            dma((1,)),
            dma((1,)),
            dma((1,)),
            dma((BLOCK - 1,)),
            dma((BLOCK - 1,)),
            dma((BLOCK,)),
            dma((1,)),
        ],
        compiler_params=pltpu.CompilerParams(
            collective_id=0, has_side_effects=True, vmem_limit_bytes=64000 * 1024
        ),
    )(*small, *big)


def solution(mesh):
    in_specs = (
        P("ep", "tp"),
        P("ep", "tp"),
        P("ep", "tp"),
        P("tp", "ep"),
        P("tp", "ep"),
        P("ep", "tp"),
        P("tp"),
        P(None, "tp"),
        P("ep", "tp"),
        P("ep", None),
        P("ep", None),
        P("ep", "tp", None),
        P("ep", "tp", None),
        P("ep", None, "tp"),
    )
    out_specs = (P("ep", "tp"), P("ep", "tp"))
    return jax.shard_map(body, mesh=mesh, in_specs=in_specs, out_specs=out_specs, check_vma=False)
```

```python
import functools

import jax
import jax.numpy as jnp
from jax import lax
from jax.experimental import pallas as pl
from jax.experimental.pallas import tpu as pltpu
from jax.sharding import PartitionSpec as P

EPSILON = 1e-06
LOG_FLOOR = -1e30
F32 = jnp.float32
BF16 = jnp.bfloat16
GROUPS = 8
SIDE = 4
PARTS = 4
BLOCK = 4
HEAD = 8
LABEL = 16
SEQUENCE = (
    "s00", "d0", "s01", "s10", "s20", "s02", "s11", "near", "s30", "s21", "s40", "s12", "s50",
    "s03", "s31", "s70", "s60", "s22", "carry1", "s13", "s51", "s32", "h0", "s04", "s41", "up",
    "s23", "carry2", "s61", "s14", "s33", "s05", "s24", "s71", "s42", "s52", "s62", "s15",
    "heads", "s34", "s06", "g0", "s43", "s72", "s25", "s16", "g1", "s53", "g3", "s63", "d1",
    "s44", "s35", "s26", "s54", "s73", "r0", "s45", "r3", "s36", "s64", "s55", "r1", "h1",
    "s74", "g2", "m0", "s46", "s65", "m1", "s56", "s75", "r2", "m3", "s66", "s76", "m2", "b0",
    "b2", "b1", "f0", "b4", "b3", "f3", "f1", "f2", "b5", "b6", "b7",
)
TURNED = ()
ORDER = (0, 8, 7, -7, 6, -6, 5, -5, 4, -4, 3, -3, 2, -2, 1, -1)


def flip(index, bits):
    place = 1
    while place <= bits:
        if bits & place:
            index = index + place * (1 - 2 * ((index // place) % 2))
        place *= 2
    return index


def dot(left, right, contract=((1,), (0,))):
    return lax.dot_general(left, right, (contract, ((), ())), preferred_element_type=F32)


def own_mask(size):
    return lax.broadcasted_iota(jnp.int32, (size, size), 0) == lax.broadcasted_iota(
        jnp.int32, (size, size), 1
    )


def upright(row):
    size = row.shape[1]
    return jnp.sum(jnp.where(own_mask(size), row, 0.0), axis=1, keepdims=True)


def flat(column):
    size = column.shape[0]
    return jnp.sum(jnp.where(own_mask(size), column, 0.0), axis=0, keepdims=True)


def kernel(
    ep,
    tp,
    model_width,
    x_hbm,
    routes_hbm,
    weight_hbm,
    in_hbm,
    forget_hbm,
    gain_hbm,
    q_hbm,
    k_hbm,
    v_hbm,
    og_hbm,
    wg_hbm,
    wu_hbm,
    wd_hbm,
    wm_hbm,
    mix_ref,
    exp_ref,
    x_ref,
    routes_ref,
    weight_ref,
    in_ref,
    forget_ref,
    gain_ref,
    q_ref,
    k_ref,
    v_ref,
    og_ref,
    wd_ref,
    slot_row_ref,
    a_ref,
    cum_ref,
    w1,
    wmix,
    w2,
    slots,
    tok,
    part_own,
    part_out,
    part_in,
    sq_out,
    sq_in,
    hid,
    outb,
    ret,
    total_ref,
    hm,
    mix_own,
    mix_out,
    mix_in,
    num_ref,
    den_ref,
    top_ref,
    loc,
    pair_in,
    both,
    earlier,
    other,
    prior,
    down_in,
    near_out,
    near_in,
    carry_out,
    carry_in,
    load_sem,
    own_sem,
    deal_send,
    deal_recv,
    mix_deal_send,
    mix_deal_recv,
    hand_send,
    hand_recv,
    disp_send,
    disp_recv,
    tok_send,
    tok_recv,
    part_send,
    part_recv,
    sq_send,
    sq_recv,
    hid_send,
    hid_recv,
    ret_send,
    ret_recv,
    head_send,
    head_recv,
    mix_send,
    mix_recv,
    pair_send,
    pair_recv,
    down_send,
    down_recv,
    near_send,
    near_recv,
    carry_send,
    carry_recv,
):
    me = lax.axis_index("ep")
    mine = lax.axis_index("tp")
    row, column = mine // SIDE, mine % SIDE
    chip, core = me // 2, me % 2
    chips = ep // 2
    block, place_in_block = chip // BLOCK, chip % BLOCK
    last_block = chips // BLOCK - 1
    cap = slots.shape[0] // ep
    span = slots.shape[0] // GROUPS
    half_span = span // 2
    per = ep // GROUPS
    width = x_ref.shape[1]
    tokens = x_ref.shape[0]
    length, qk = q_ref.shape
    vw = v_ref.shape[1]
    units = wg_hbm.shape[0]
    wide = SIDE * width

    names = (
        (routes_hbm, routes_ref),
        (x_hbm, x_ref),
        (forget_hbm, forget_ref),
        (in_hbm, in_ref),
        (k_hbm, k_ref),
        (v_hbm, v_ref),
        (q_hbm, q_ref),
        (wd_hbm, wd_ref),
        (og_hbm, og_ref),
        (gain_hbm, gain_ref),
        (weight_hbm, weight_ref),
    )
    loads = [
        pltpu.make_async_copy(source, target, load_sem.at[at])
        for at, (source, target) in enumerate(names)
    ]
    for load in loads:
        load.start()

    def piece(source, j, k):
        start = pl.multiple_of((flip(row, k) * SIDE + flip(column, j)) * width, width)
        return source.at[:, pl.ds(start, width)]

    def slot_of(j, which, k):
        return w1.at[pl.ds((2 * j + which) * units, units), pl.ds(k * width, width)]

    own_pieces = [
        pltpu.make_async_copy(
            piece(source, 0, k), slot_of(0, which, k), own_sem.at[which * SIDE + k]
        )
        for which, source in enumerate((wg_hbm, wu_hbm))
        for k in range(SIDE)
    ]

    def mix_piece(j, k):
        turned = row + (k % 2) * (1 - 2 * (row % 2)) + 2 * (k // 2) * (1 - 2 * (row // 2 % 2))
        start = pl.multiple_of((turned * SIDE + flip(column, j)) * width, width)
        return wm_hbm.at[pl.ds(start, width), :]

    def mix_slot(j, k):
        return wmix.at[pl.ds(pl.multiple_of(k * width, width), width), pl.ds(j * width, width)]

    own_pieces += [
        pltpu.make_async_copy(mix_piece(0, k), mix_slot(0, k), own_sem.at[2 * SIDE + k])
        for k in range(SIDE)
    ]
    for load in own_pieces:
        load.start()


    def deal_mix(j, at):
        k = core + 2 * at
        return pltpu.make_async_remote_copy(
            mix_piece(j, k),
            mix_slot(j, k),
            mix_deal_send.at[0],
            mix_deal_recv.at[at],
            device_id={"tp": flip(mine, j)},
        )

    def foreign_rows(k):
        start = pl.multiple_of(k * width, width)
        return wmix.at[pl.ds(start, width), pl.ds(width, (SIDE - 1) * width)]

    def mix_dealt(at):
        foreign = foreign_rows(core + 2 * at)
        return pltpu.make_async_remote_copy(
            foreign, foreign, mix_deal_send.at[0], mix_deal_recv.at[at], device_id={"tp": flip(mine, 1)}
        )

    def hand_mix(at, whose):
        foreign = foreign_rows(whose + 2 * at)
        return pltpu.make_async_remote_copy(
            foreign, foreign, hand_send.at[at], hand_recv.at[at], device_id={"ep": flip(me, 1)}
        )

    def deal(j, which, k):
        return pltpu.make_async_remote_copy(
            piece(wu_hbm if which else wg_hbm, j, k),
            slot_of(j, which, k),
            deal_send.at[0],
            deal_recv.at[0],
            device_id={"tp": flip(mine, j)},
        )

    def deals():
        foreign = w1.at[pl.ds(2 * units, 2 * (SIDE - 1) * units)]
        return pltpu.make_async_remote_copy(
            foreign, foreign, deal_send.at[0], deal_recv.at[0], device_id={"tp": flip(mine, 1)}
        )

    dealt = [(j, which, k) for j in range(1, SIDE) for which in range(2) for k in range(SIDE)]

    barrier = pltpu.get_barrier_semaphore()
    for i in range(1, ep):
        pl.semaphore_signal(barrier, inc=1, device_id={"ep": flip(me, i)})
    for j in range(1, tp):
        pl.semaphore_signal(barrier, inc=1, device_id={"tp": flip(mine, j)})

    loads[0].wait()
    experts = lax.broadcasted_iota(jnp.int32, (ep, tokens), 0)

    offsets = ORDER if chips == len(ORDER) else tuple(range(chips))

    def turn_of(expert):
        ahead = ((expert >> 1) - chip) & (chips - 1)
        step = jnp.zeros_like(ahead)
        for at, ahead_of in enumerate(offsets):
            step = jnp.where(ahead == ahead_of % chips, at, step)
        return 2 * step + ((expert & 1) ^ core)

    named = [experts == turn_of(routes_ref[route : route + 1, :]) for route in range(2)]
    any_named = (named[0] | named[1]).astype(F32).astype(BF16)
    older = lax.broadcasted_iota(jnp.int32, (tokens, tokens), 0) < lax.broadcasted_iota(
        jnp.int32, (tokens, tokens), 1
    )
    before = dot(any_named, older.astype(F32).astype(BF16))
    places = (experts * cap).astype(F32) + before
    for route in range(2):
        slot_row_ref[route : route + 1, :] = jnp.sum(
            jnp.where(named[route], places, 0.0), axis=0, keepdims=True
        ).astype(jnp.int32)
    loads[1].wait()

    def pick(group, carry):
        at = group * span
        rows = at + lax.broadcasted_iota(jnp.int32, (span, tokens), 0)
        hit = (rows == slot_row_ref[0:1, :]) | (rows == slot_row_ref[1:2, :])
        chosen = dot(hit.astype(F32).astype(BF16), x_ref[...]).astype(BF16)
        slots[pl.ds(pl.multiple_of(at, span), span), :] = chosen
        return carry

    lax.fori_loop(0, GROUPS, pick, 0)

    with jax.named_scope("barrier"):
        pl.semaphore_wait(barrier, ep - 1 + tp - 1)

    def peer(i, sign):
        return 2 * ((chip + sign * offsets[i // 2] + chips) % chips) + (core + i) % 2

    def dispatch(i):
        return pltpu.make_async_remote_copy(
            slots.at[pl.ds(i * cap, cap)],
            tok.at[pl.ds(i * cap, cap), pl.ds(0, width)],
            disp_send.at[0],
            disp_recv.at[i // per],
            device_id={"ep": peer(i, 1)},
        )

    def dispatched(group):
        begin = cap if group == 0 else group * span
        rows = pl.ds(begin, (group + 1) * span - begin)
        return pltpu.make_async_remote_copy(
            slots.at[rows],
            tok.at[rows, pl.ds(0, width)],
            disp_send.at[0],
            disp_recv.at[group],
            device_id={"ep": flip(me, 1)},
        )

    for i in range(1, ep // 2):
        dispatch(i).start()

    tok[0:cap, 0:width] = slots[0:cap, :]
    for each in dealt:
        deal(*each).start()


    loads[2].wait()
    loads[3].wait()
    gates_in = forget_ref[...]
    log_keep = jnp.minimum(gates_in, 0.0) - jnp.log1p(jnp.exp(-jnp.abs(gates_in)))
    high = log_keep.astype(BF16).astype(F32)
    mid = (log_keep - high).astype(BF16).astype(F32)
    low = log_keep - high - mid
    which_row = lax.broadcasted_iota(jnp.int32, (8, length), 0)
    thirds = jnp.where(
        which_row == 0, high, jnp.where(which_row == 1, mid, jnp.where(which_row == 2, low, 0.0))
    )
    upto = lax.broadcasted_iota(jnp.int32, (length, length), 0) <= lax.broadcasted_iota(
        jnp.int32, (length, length), 1
    )
    sums = dot(thirds.astype(BF16), upto.astype(F32).astype(BF16))
    cum_ref[...] = sums[0:1, :] + sums[1:2, :] + sums[2:3, :]
    a_ref[...] = in_ref[...] - cum_ref[...]

    loads[4].wait()
    loads[5].wait()
    decay = cum_ref[0:1, length - 1 : length]
    log_in = a_ref[0:1, :]
    local_top = jnp.max(log_in, axis=1, keepdims=True)
    weighted = k_ref[...].astype(F32) * jnp.exp(upright(log_in) - local_top)
    loc[HEAD : HEAD + qk, :] = dot(weighted.astype(BF16), v_ref[...], ((0,), (0,)))
    loc[0:HEAD, 0:qk] = jnp.broadcast_to(jnp.sum(weighted, axis=0, keepdims=True), (HEAD, qk))
    loc[0:HEAD, qk:vw] = jnp.broadcast_to(local_top + decay, (HEAD, vw - qk))
    loc[HEAD + qk :, :] = jnp.broadcast_to(decay, (8, vw))

    pair = pltpu.make_async_remote_copy(
        loc, pair_in, pair_send.at[0], pair_recv.at[0], device_id={"ep": flip(me, 1)}
    )

    @pl.when(core == 0)
    def _():
        pair.start()

    def gates(first_max, second_max):
        top = jnp.maximum(first_max, second_max)
        return top, jnp.exp(first_max - top), jnp.exp(second_max - top)

    def merge(target, first, second):
        second_decay = second[HEAD + qk : HEAD + qk + 1, 0:1]
        top, keep, add = gates(
            first[0:1, qk : qk + 1] + second_decay, second[0:1, qk : qk + 1]
        )
        target[0:HEAD, 0:qk] = keep * first[0:HEAD, 0:qk] + add * second[0:HEAD, 0:qk]
        target[0:HEAD, qk:vw] = jnp.broadcast_to(top, (HEAD, vw - qk))
        target[HEAD : HEAD + qk, :] = (
            keep * first[HEAD : HEAD + qk, :] + add * second[HEAD : HEAD + qk, :]
        )
        target[HEAD + qk :, :] = first[HEAD + qk :, :] + second[HEAD + qk :, :]


    def encode(target, source):
        line = lax.broadcasted_iota(jnp.int32, (LABEL, vw), 0)
        label = jnp.zeros((LABEL, vw), F32)
        for base, rest in ((0, source[0:1, :]), (3, source[HEAD + qk : HEAD + qk + 1, :])):
            for at in range(3):
                part = rest.astype(BF16).astype(F32)
                label = jnp.where(line == base + at, part, label)
                rest = rest - part
        target[0:LABEL, :] = label.astype(BF16)
        target[LABEL:, :] = source[HEAD : HEAD + qk, :].astype(BF16)

    def decode(target, source):
        label = source[0:LABEL, :].astype(F32)
        target[0:HEAD, :] = jnp.broadcast_to(label[0:1, :] + label[1:2, :] + label[2:3, :], (HEAD, vw))
        target[HEAD + qk :, :] = jnp.broadcast_to(
            label[3:4, :] + label[4:5, :] + label[5:6, :], (8, vw)
        )
        target[HEAD : HEAD + qk, :] = source[LABEL:, :].astype(F32)

    def near(ahead):
        return pltpu.make_async_remote_copy(
            near_out,
            near_in.at[ahead - 1],
            near_send.at[ahead - 1],
            near_recv.at[ahead - 1],
            device_id={"ep": me + 2 * ahead},
        )

    def carry(ahead):
        return pltpu.make_async_remote_copy(
            carry_out,
            carry_in,
            carry_send.at[ahead - 1],
            carry_recv.at[0],
            device_id={"ep": me + 2 * ahead},
        )

    down = pltpu.make_async_remote_copy(
        other, down_in, down_send.at[0], down_recv.at[0], device_id={"ep": flip(me, 1)}
    )

    @pl.when(core == 1)
    def _():
        pair.wait_recv()
        merge(both, pair_in, loc)
        encode(near_out, both)
        for ahead in range(BLOCK - 1, 0, -1):

            @pl.when(place_in_block + ahead < BLOCK)
            def _():
                near(ahead).start()

    for i in range(ep // 2, ep):
        dispatch(i).start()

    def gather_block():
        earlier[0:HEAD, 0:qk] = jnp.zeros((HEAD, qk), F32)
        earlier[0:HEAD, qk:vw] = jnp.full((HEAD, vw - qk), LOG_FLOOR, F32)
        earlier[HEAD:, :] = jnp.zeros((qk + 8, vw), F32)
        for ahead in range(BLOCK - 1, 0, -1):

            @pl.when(place_in_block >= ahead)
            def _():
                near(ahead).wait_recv()
                decode(other, near_in.at[ahead - 1])
                merge(earlier, earlier, other)

    sends_carry = (core == 1) & (place_in_block == BLOCK - 1) & (block < last_block)

    def take_carry():
        carry(1).wait_recv()
        decode(other, carry_in)

    def send_carry(number):
        @pl.when(sends_carry & (block == number))
        def _():
            with jax.named_scope("carry"):
                if number > 0:
                    take_carry()
                    merge(other, other, earlier)
                    merge(prior, other, both)
                else:
                    merge(prior, earlier, both)
                encode(carry_out, prior)
                for ahead in range(BLOCK, 0, -1):
                    carry(ahead).start()

    with jax.named_scope("inblock"):
        loads[6].wait()
    tile = length // 4
    scale = qk**-0.5
    for at in range(4):
        rows = pl.ds(at * tile, tile)
        seen = (at + 1) * tile
        causal = lax.broadcasted_iota(jnp.int32, (tile, seen), 1) <= at * tile + (
            lax.broadcasted_iota(jnp.int32, (tile, seen), 0)
        )
        log_seen = jnp.where(causal, a_ref[0:1, 0:seen], -jnp.inf)
        top = jnp.max(log_seen, axis=1, keepdims=True)
        scores = dot(q_ref[rows, :], k_ref[0:seen, :], ((1,), (1,))) * scale
        scores = scores * jnp.exp(log_seen - top)
        num_ref[rows, :] = dot(scores.astype(BF16), v_ref[0:seen, :])
        den_ref[rows, :] = jnp.broadcast_to(jnp.sum(scores, axis=1, keepdims=True), (tile, 128))
        top_ref[rows, :] = jnp.broadcast_to(top, (tile, 128))


    def build_down():
        loads[7].wait()
        nothing = jnp.zeros((units, width), BF16)
        for turned in range(2 if TURNED else 1):
            for at in range(tp):
                unit = (at % SIDE) * SIDE + at // SIDE if turned else at
                kept = wd_ref[unit * units : (unit + 1) * units, :]
                first = at * 2 * units
                w2[turned, first : first + units, 0:width] = kept
                w2[turned, first : first + units, width : 2 * width] = nothing
                w2[turned, first + units : first + 2 * units, 0:width] = nothing
                w2[turned, first + units : first + 2 * units, width : 2 * width] = kept


    def spread(group, k):
        rows = pl.ds(group * span, span)
        return pltpu.make_async_remote_copy(
            tok.at[rows, pl.ds(0, width)],
            tok.at[rows, pl.ds(k * width, width)],
            tok_send.at[0],
            tok_recv.at[group, k // 2],
            device_id={"tp": flip(mine, SIDE * k)},
        )

    def onward(group, k):
        rows = pl.ds(group * span + (k // 2) * half_span, half_span)
        return pltpu.make_async_remote_copy(
            tok.at[rows, pl.ds(k * width, width)],
            tok.at[rows, pl.ds(2 * width, width)],
            tok_send.at[0],
            tok_recv.at[group, 2 + k // 2],
            device_id={"tp": flip(mine, SIDE * (SIDE - k))},
        )

    def send_partial(group, j):
        rows = pl.ds(group * span, span)
        return pltpu.make_async_remote_copy(
            part_out.at[j, rows],
            part_in.at[j, rows],
            part_send.at[0],
            part_recv.at[group],
            device_id={"tp": flip(mine, j)},
        )

    def send_squares(group, j):
        return pltpu.make_async_remote_copy(
            sq_out.at[group],
            sq_in.at[group, j],
            sq_send.at[0],
            sq_recv.at[group],
            device_id={"tp": flip(mine, j)},
        )

    def partials(group):
        rows = pl.ds(group * span, span)
        return pltpu.make_async_remote_copy(
            part_out.at[pl.ds(1, SIDE - 1), rows],
            part_in.at[pl.ds(1, SIDE - 1), rows],
            part_send.at[0],
            part_recv.at[group],
            device_id={"tp": flip(mine, 1)},
        )

    def squares_of(group):
        foreign = sq_in.at[group, pl.ds(1, SIDE - 1)]
        return pltpu.make_async_remote_copy(
            foreign, foreign, sq_send.at[0], sq_recv.at[group], device_id={"tp": flip(mine, 1)}
        )


    def hid_block(group, at, count):
        return hid.at[
            pl.ds(group * half_span, half_span),
            pl.ds(pl.multiple_of(at * 2 * units, 2 * units), count * 2 * units),
        ]

    def axes_of(group):
        return (row, column, SIDE, 1) if group in TURNED else (column, row, 1, SIDE)

    def hid_inner(group, k):
        inner, outer, stride, _ = axes_of(group)
        block_of = hid_block(group, outer * SIDE + inner, 1)
        return pltpu.make_async_remote_copy(
            block_of, block_of, hid_send.at[0], hid_recv.at[group, 0], device_id={"tp": flip(mine, stride * k)}
        )

    def hid_outer(group, k):
        _, outer, _, stride = axes_of(group)
        block_of = hid_block(group, outer * SIDE, SIDE)
        return pltpu.make_async_remote_copy(
            block_of,
            block_of,
            hid_send.at[0],
            hid_recv.at[group, 1 + k // 2],
            device_id={"tp": flip(mine, stride * k)},
        )

    def hid_onward(group, k):
        _, outer, _, stride = axes_of(group)
        quarter = half_span // 2
        block_of = hid.at[
            pl.ds(group * half_span + (k // 2) * quarter, quarter),
            pl.ds(
                pl.multiple_of(flip(outer, k) * SIDE * 2 * units, SIDE * 2 * units), SIDE * 2 * units
            ),
        ]
        return pltpu.make_async_remote_copy(
            block_of,
            block_of,
            hid_send.at[0],
            hid_recv.at[group, 3 + k // 2],
            device_id={"tp": flip(mine, stride * (SIDE - k))},
        )

    def hid_row(group):
        foreign = hid_block(group, 0, SIDE - 1)
        return pltpu.make_async_remote_copy(
            foreign, foreign, hid_send.at[0], hid_recv.at[group, 0], device_id={"tp": flip(mine, 1)}
        )

    def give_back(i):
        return pltpu.make_async_remote_copy(
            outb.at[pl.ds(i * cap, cap)],
            ret.at[pl.ds(i * cap, cap)],
            ret_send.at[0],
            ret_recv.at[i // per],
            device_id={"ep": peer(i, -1)},
        )

    def given_back(group):
        begin = cap if group == 0 else group * span
        rows = pl.ds(begin, (group + 1) * span - begin)
        return pltpu.make_async_remote_copy(
            outb.at[rows], ret.at[rows], ret_send.at[0], ret_recv.at[group], device_id={"ep": flip(me, 1)}
        )

    def stage(group, step):
        rows = pl.ds(group * span, span)
        packed = pl.ds(group * half_span, half_span)
        if step == 0:
            dispatched(group).wait_recv()
            for k in (1, 3):
                spread(group, k).start()
        elif step == 1:
            for k in (1, 3):
                spread(group, k).wait_recv()
                onward(group, k).start()
        elif step == 2:
            if group == 0:
                for load in own_pieces[0 : 2 * SIDE]:
                    load.wait()
                deals().wait_recv()
            for k in (1, 3):
                onward(group, k).wait_recv()
            piece_of = tok[rows, :]
            partial = dot(piece_of, w1[...], ((1,), (1,)))
            part_own[rows, :] = partial[:, 0 : 2 * units]
            for j in range(1, SIDE):
                part_out[j, rows, :] = partial[:, j * 2 * units : (j + 1) * 2 * units].astype(BF16)
            for j in range(1, SIDE):
                send_partial(group, j).start()
            full = piece_of.astype(F32)
            squares = flat(jnp.sum(full * full, axis=1, keepdims=True))
            sq_out[group] = jnp.broadcast_to(squares, (8, span))
            for j in range(1, SIDE):
                send_squares(group, j).start()
        elif step == 3:
            squares = sq_out[group][0:1, :]
            squares_of(group).wait_recv()
            for j in range(1, SIDE):
                squares = squares + sq_in[group, j][0:1, :]
            inverse = upright(lax.rsqrt(squares / model_width + EPSILON))
            total = part_own[rows, :]
            partials(group).wait_recv()
            for j in range(1, SIDE):
                total = total + part_in[j, rows, :].astype(F32)
            total = total * inverse
            hidden = jax.nn.silu(total) * pltpu.roll(total, units, 1)
            turned = pltpu.roll(hidden, units, 1)
            lanes = lax.broadcasted_iota(jnp.int32, (half_span, 2 * units), 1)
            both_rows = jnp.where(lanes < units, hidden[0:half_span, :], turned[half_span:span, :])
            inner, outer, _, _ = axes_of(group)
            place = outer * SIDE + inner
            columns = pl.ds(pl.multiple_of(place * 2 * units, 2 * units), 2 * units)
            hid[packed, columns] = both_rows.astype(BF16)
            for k in range(1, SIDE):
                hid_inner(group, k).start()
        elif step == 4:
            hid_row(group).wait_recv()
            for k in (1, 3):
                hid_outer(group, k).start()
        elif step == 5:
            for k in (1, 3):
                hid_outer(group, k).wait_recv()
                hid_onward(group, k).start()
        else:
            for k in (1, 3):
                hid_onward(group, k).wait_recv()
            total = dot(hid[packed, :], w2[int(group in TURNED)])
            outb[pl.ds(group * span, half_span), :] = total[:, 0:width].astype(BF16)
            outb[pl.ds(group * span + half_span, half_span), :] = total[:, width:].astype(BF16)
            for i in range(max(1, group * per), (group + 1) * per):
                give_back(i).start()
            if group == 0:
                ret[0:cap, :] = outb[0:cap, :]

    part_rows = length // PARTS

    def head_spread(at, k):
        rows = pl.ds(at * part_rows, part_rows)
        return pltpu.make_async_remote_copy(
            hm.at[rows, pl.ds(0, width)],
            hm.at[rows, pl.ds(k * width, width)],
            head_send.at[0],
            head_recv.at[at, k // 2],
            device_id={"tp": flip(mine, SIDE * k)},
        )

    def head_onward(at, k):
        half = part_rows // 2
        rows = pl.ds(at * part_rows + (k // 2) * half, half)
        return pltpu.make_async_remote_copy(
            hm.at[rows, pl.ds(k * width, width)],
            hm.at[rows, pl.ds(2 * width, width)],
            head_send.at[0],
            head_recv.at[at, 2 + k // 2],
            device_id={"tp": flip(mine, SIDE * (SIDE - k))},
        )

    def relay_heads(at):
        for k in (1, 3):
            head_spread(at, k).wait_recv()
            head_onward(at, k).start()

    def mix_partial(at, j):
        rows = pl.ds(at * part_rows, part_rows)
        return pltpu.make_async_remote_copy(
            mix_out.at[j, rows],
            mix_in.at[j, rows],
            mix_send.at[0],
            mix_recv.at[at],
            device_id={"tp": flip(mine, j)},
        )

    def mix_partials(at):
        foreign = mix_in.at[pl.ds(1, SIDE - 1), pl.ds(at * part_rows, part_rows)]
        return pltpu.make_async_remote_copy(
            foreign, foreign, mix_send.at[0], mix_recv.at[at], device_id={"tp": flip(mine, 1)}
        )


    def take_prior():
        @pl.when(core == 1)
        def _():
            @pl.when((block > 0) & jnp.logical_not(sends_carry))
            def _():
                take_carry()
                merge(other, other, earlier)

            @pl.when(block == 0)
            def _():
                other[...] = earlier[...]

            down.start()
            merge(prior, other, pair_in)

        @pl.when(core == 0)
        def _():
            down.wait_recv()
            prior[...] = down_in[...]

        for load in loads[8:10]:
            load.wait()

    def finish_heads(at):
        prior_max = prior[0:1, qk : qk + 1]
        normal = prior[0:1, 0:qk]
        memory = prior[HEAD : HEAD + qk, :]
        high = memory.astype(BF16)
        low = (memory - high.astype(F32)).astype(BF16)
        rows = pl.ds(at * part_rows, part_rows)
        queries = q_ref[rows, :]
        own_top = top_ref[rows, 0:1]
        top = jnp.maximum(prior_max, own_top)
        again = jnp.exp(own_top - top)
        carried = jnp.exp(prior_max - top) * scale
        numerator = carried * (dot(queries, high) + dot(queries, low)) + again * num_ref[rows, :]
        denominator = (
            carried * jnp.sum(queries.astype(F32) * normal, axis=1, keepdims=True)
            + again * den_ref[rows, 0:1]
        )
        cumulative = upright(cum_ref[0:1, at * part_rows : (at + 1) * part_rows])
        floor = jnp.exp(-(cumulative + top))
        value = numerator / jnp.maximum(jnp.abs(denominator), floor)
        value = value * lax.rsqrt(jnp.mean(value * value, axis=1, keepdims=True) + EPSILON)
        gate = jax.nn.sigmoid(og_ref[rows, :].astype(F32))
        hm[rows, 0:width] = (value * gain_ref[...] * gate).astype(BF16)
        for k in (1, 3):
            head_spread(at, k).start()

    def mix_step(at):
        if at == first_mixed:
            for load in own_pieces[2 * SIDE :]:
                load.wait()
            for half in range(2):
                hand_mix(half, 1 - core).wait_recv()
        for k in (1, 3):
            head_onward(at, k).wait_recv()
        rows = pl.ds(at * part_rows, part_rows)
        partial = dot(hm[rows, :], wmix[...])
        mix_own[rows, :] = partial[:, 0:width]
        for j in range(1, SIDE):
            mix_out[j, rows, :] = partial[:, j * width : (j + 1) * width].astype(BF16)
        for j in range(1, SIDE):
            mix_partial(at, j).start()

    def mix_finish(at):
        mix_partials(at).wait_recv()
        rows = pl.ds(at * part_rows, part_rows)
        total = mix_own[rows, :]
        for j in range(1, SIDE):
            total = total + mix_in[j, rows, :].astype(F32)
        mix_ref[rows, :] = total.astype(BF16)

    def near_step():
        @pl.when(core == 1)
        def _():
            gather_block()

        send_carry(0)

    first_back = min((SEQUENCE.index(f"b{at}"), at) for at in range(GROUPS))[1]
    first_mixed = min((SEQUENCE.index(f"m{at}"), at) for at in range(PARTS))[1]

    def deal_step(at):
        for j in range(1, SIDE):
            deal_mix(j, at).start()

    def hand_step(at):
        mix_dealt(at).wait_recv()
        hand_mix(at, core).start()

    def back_step(group):
        if group == first_back:
            loads[10].wait()
        given_back(group).wait_recv()
        rows = pl.ds(group * span, span)
        places = lax.broadcasted_iota(jnp.int32, (span, tokens), 0)
        for route in range(2):
            hit = places == slot_row_ref[route : route + 1, :] - group * span
            picked = dot(hit.astype(F32).astype(BF16), ret[rows, :], ((0,), (0,)))
            picked = picked * upright(weight_ref[route : route + 1, :])
            if group == first_back and route == 0:
                total_ref[...] = picked
            else:
                total_ref[...] += picked

    named_steps = {
        "near": near_step,
        "heads": take_prior,
        "up": build_down,
        "carry1": lambda: send_carry(1),
        "carry2": lambda: send_carry(2),
    }
    for item in SEQUENCE:
        with jax.named_scope(item):
            if item in named_steps:
                named_steps[item]()
            elif item[0] == "s":
                stage(int(item[1]), int(item[2]))
            elif item[0] == "d":
                deal_step(int(item[1]))
            elif item[0] == "h" and item != "heads":
                hand_step(int(item[1]))
            elif item[0] == "b":
                back_step(int(item[1]))
            elif item[0] == "g":
                finish_heads(int(item[1]))
            elif item[0] == "r":
                relay_heads(int(item[1]))
            elif item[0] == "m":
                mix_step(int(item[1]))
            else:
                mix_finish(int(item[1]))
    exp_ref[...] = total_ref[...].astype(BF16)

    def sent(source, semaphore):
        pltpu.make_async_remote_copy(
            source, source, semaphore, semaphore, device_id={"ep": flip(me, 1)}
        ).wait_send()

    with jax.named_scope("drain"):
        foreign = pl.ds(cap, slots.shape[0] - cap)
        sent(slots.at[foreign], disp_send.at[0])
        sent(outb.at[foreign], ret_send.at[0])
        deals().wait_send()
        sent(tok.at[:, pl.ds(0, 3 * width)], tok_send.at[0])
        for half in range(2):
            mix_dealt(half).wait_send()
            hand_mix(half, core).wait_send()
        sent(part_out.at[pl.ds(1, SIDE - 1)], part_send.at[0])
        sent(sq_in.at[:, pl.ds(1, SIDE - 1)], sq_send.at[0])
        sent(hid.at[:, pl.ds(0, (tp - 1) * 2 * units)], hid_send.at[0])
        sent(hm.at[:, pl.ds(0, (SIDE - 1) * width)], head_send.at[0])
        sent(mix_in.at[pl.ds(1, SIDE - 1)], mix_send.at[0])

    @pl.when(core == 0)
    def _():
        pair.wait_send()

    @pl.when(core == 1)
    def _():
        down.wait_send()
        for ahead in range(1, BLOCK):

            @pl.when(place_in_block + ahead < BLOCK)
            def _():
                near(ahead).wait_send()

    @pl.when(sends_carry)
    def _():
        for ahead in range(1, BLOCK + 1):
            carry(ahead).wait_send()


def body(
    query_rows,
    key_rows,
    value_rows,
    in_gate,
    forget_gate,
    out_gate,
    head_gain,
    mix_weight,
    expert_input,
    routes,
    route_weight,
    gate_weight,
    up_weight,
    down_weight,
):
    ep, tp = lax.axis_size("ep"), lax.axis_size("tp")
    length = in_gate.shape[1]
    token_count, fanout = routes.shape
    width = expert_input.shape[1]
    units = gate_weight.shape[1]
    capacity = 2 * token_count * fanout // ep
    slot_count = ep * capacity
    qk = query_rows.shape[1]
    vw = value_rows.shape[1]

    vmem = pl.BlockSpec(memory_space=pltpu.VMEM)
    anywhere = pl.BlockSpec(memory_space=pl.ANY)
    dma = pltpu.SemaphoreType.DMA
    gate_local, up_local, down_local = gate_weight[0], up_weight[0], down_weight[0]
    small = (expert_input, routes.T, route_weight.T, in_gate, forget_gate, head_gain[None, :])
    big = (query_rows, key_rows, value_rows, out_gate, gate_local, up_local, down_local, mix_weight)
    held = (query_rows, key_rows, value_rows, out_gate, down_local)
    tall = (HEAD + qk + 8, vw)
    message = (LABEL + qk, vw)
    results = pl.pallas_call(
        functools.partial(kernel, ep, tp, mix_weight.shape[0]),
        out_shape=(
            pltpu.VMEM((length, width), BF16),
            pltpu.VMEM((token_count, width), BF16),
        ),
        in_specs=[anywhere] * 14,
        out_specs=(vmem, vmem),
        scratch_shapes=[pltpu.VMEM(array.shape, array.dtype) for array in small + held]
        + [
            pltpu.VMEM((fanout, token_count), jnp.int32),
            pltpu.VMEM((1, length), F32),
            pltpu.VMEM((1, length), F32),
            pltpu.VMEM((SIDE * 2 * units, SIDE * width), BF16),
            pltpu.VMEM((SIDE * width, SIDE * width), BF16),
            pltpu.VMEM((2 if TURNED else 1, tp * 2 * units, 2 * width), BF16),
            pltpu.VMEM((slot_count, width), BF16),
            pltpu.VMEM((slot_count, SIDE * width), BF16),
            pltpu.VMEM((slot_count, 2 * units), F32),
            pltpu.VMEM((SIDE, slot_count, 2 * units), BF16),
            pltpu.VMEM((SIDE, slot_count, 2 * units), BF16),
            pltpu.VMEM((GROUPS, 8, slot_count // GROUPS), F32),
            pltpu.VMEM((GROUPS, SIDE, 8, slot_count // GROUPS), F32),
            pltpu.VMEM((slot_count // 2, tp * 2 * units), BF16),
            pltpu.VMEM((slot_count, width), BF16),
            pltpu.VMEM((slot_count, width), BF16),
            pltpu.VMEM((token_count, width), F32),
            pltpu.VMEM((length, SIDE * width), BF16),
            pltpu.VMEM((length, width), F32),
            pltpu.VMEM((SIDE, length, width), BF16),
            pltpu.VMEM((SIDE, length, width), BF16),
            pltpu.VMEM((length, vw), F32),
            pltpu.VMEM((length, 128), F32),
            pltpu.VMEM((length, 128), F32),
            pltpu.VMEM(tall, F32),
            pltpu.VMEM(tall, F32),
            pltpu.VMEM(tall, F32),
            pltpu.VMEM(tall, F32),
            pltpu.VMEM(tall, F32),
            pltpu.VMEM(tall, F32),
            pltpu.VMEM(tall, F32),
            pltpu.VMEM(message, BF16),
            pltpu.VMEM((BLOCK - 1, *message), BF16),
            pltpu.VMEM(message, BF16),
            pltpu.VMEM(message, BF16),
            dma((11,)),
            dma((3 * SIDE,)),
            dma((1,)),
            dma((1,)),
            dma((1,)),
            dma((2,)),
            dma((2,)),
            dma((2,)),
            dma((1,)),
            dma((GROUPS,)),
            dma((1,)),
            dma((GROUPS, 4)),
            dma((1,)),
            dma((GROUPS,)),
            dma((1,)),
            dma((GROUPS,)),
            dma((1,)),
            dma((GROUPS, 5)),
            dma((1,)),
            dma((GROUPS,)),
            dma((1,)),
            dma((PARTS, 4)),
            dma((1,)),
            dma((PARTS,)),
            dma((1,)),
            dma((1,)),
            dma((1,)),
            dma((1,)),
            dma((BLOCK - 1,)),
            dma((BLOCK - 1,)),
            dma((BLOCK,)),
            dma((1,)),
        ],
        compiler_params=pltpu.CompilerParams(
            collective_id=0, has_side_effects=True, vmem_limit_bytes=64000 * 1024
        ),
    )(*small, *big)
    return results


def solution(mesh):
    in_specs = (
        P("ep", "tp"),
        P("ep", "tp"),
        P("ep", "tp"),
        P("tp", "ep"),
        P("tp", "ep"),
        P("ep", "tp"),
        P("tp"),
        P(None, "tp"),
        P("ep", "tp"),
        P("ep", None),
        P("ep", None),
        P("ep", "tp", None),
        P("ep", "tp", None),
        P("ep", None, "tp"),
    )
    out_specs = (P("ep", "tp"), P("ep", "tp"))
    return jax.shard_map(body, mesh=mesh, in_specs=in_specs, out_specs=out_specs, check_vma=False)
```
